128 devices in a mesh: sp: 64 (over z, y, x), tp: 2 (over core).
Axes of the slice: x: 4, y: 4, z: 4, core: 2. Of those that a mesh axis runs over, the one named last changes fastest.
Arguments:
- queries_narrow: bfloat16 [16384, 1024], P('sp', 'tp'), may hold values from -40 to 40
- keys_narrow: bfloat16 [16384, 256], P('sp', 'tp'), may hold values from -40 to 40
- values_narrow: bfloat16 [16384, 256], P('sp', 'tp'), may hold values from -6 to 6
- queries_wide: bfloat16 [16384, 1024], P('sp', 'tp'), may hold values from -40 to 40
- keys_wide: bfloat16 [16384, 512], P('sp', 'tp'), may hold values from -40 to 40
- values_wide: bfloat16 [16384, 512], P('sp', 'tp'), may hold values from -6 to 6
- lambda_narrow: float32 [8], P('tp'), may hold values from 0.3 to 0.8
- lambda_wide: float32 [4], P('tp'), may hold values from 0.3 to 0.8
- gain_narrow: float32 [128], replicated, may hold values from 0.1 to 1.9
- gain_wide: float32 [256], replicated, may hold values from 0.1 to 1.9
- out_narrow: bfloat16 [1024, 2048], replicated, may hold values from -0.125 to 0.125
- out_wide: bfloat16 [1024, 2048], replicated, may hold values from -0.125 to 0.125
- stream: bfloat16 [16384, 2048], P(('sp', 'tp')), may hold values from -6 to 6
- gain_mix: float32 [2048], replicated, may hold values from 0.1 to 1.9
- gain_ffn: float32 [2048], replicated, may hold values from 0.1 to 1.9
- gain_post: float32 [2048], replicated, may hold values from 0.1 to 1.9
- shared_gate: bfloat16 [2048, 512], replicated, may hold values from -0.125 to 0.125
- shared_up: bfloat16 [2048, 512], replicated, may hold values from -0.125 to 0.125
- shared_down: bfloat16 [512, 2048], replicated, may hold values from -0.25 to 0.25
- expert_gate: bfloat16 [128, 2048, 512], P('sp', None, 'tp'), may hold values from -0.125 to 0.125
- expert_up: bfloat16 [128, 2048, 512], P('sp', None, 'tp'), may hold values from -0.125 to 0.125
- expert_down: bfloat16 [128, 512, 2048], P('sp', 'tp'), may hold values from -0.25 to 0.25
- expert_ids: int32 [16384, 4], P(('sp', 'tp')), may hold values from 0 to 127, all different within a row; in each aligned block of 128 rows (0 to 127, 128 to 255, ...) at most 6 rows name the same one
- route_weights: float32 [16384, 4], P(('sp', 'tp')), may hold values from 0.2 to 1
Outputs:
- layer_out: bfloat16 [16384, 2048], P(('sp', 'tp'))
The draws below stay inside these ranges and needn't reach their ends.
Inputs may be any that keep to these rules, and one draw needn't show every extreme that they name: `expert_ids`: the experts of one token differ. Within the rows that one device holds (aligned blocks of rows in the placement's order), no expert is named more than 6 times, and in every draw some expert is named exactly 6 times there.
All inputs are finite; a program needn't handle non-finite values.
Results may differ from the reference program's by a relative error of at most 0.015.
Values may be sent and summed in bfloat16 or wider, within the bound.
A program may use at most 192 MiB of HBM per device.

```python
import math
import jax
import jax.numpy as jnp
import numpy as np
from jax import lax

D = 2048
HN = 8
DN = 64
VN = 128
KN = 2
HW = 4
DW = 128
VW = 256
KW = 2
FF = 512
SFF = 512
TOPK = 4
TOK_DEV = 256
TOKENS = 16384
EXPERTS = 128
CAP = 6
N_SP = 64
N_TP = 2


def pair_draw(key, heads, groups, key_dim, salt):
    base = jax.random.fold_in(key, salt)
    query_key, keys_key = jax.random.split(base, 2)
    queries = jax.random.normal(query_key, (TOKENS, heads, 2, key_dim), jnp.float32) * 1.4
    keys = jax.random.normal(keys_key, (TOKENS, groups, 2, key_dim), jnp.float32) * 1.3
    queries = jnp.clip(queries, -40.0, 40.0)
    keys = jnp.clip(keys, -40.0, 40.0)
    return (queries.reshape(TOKENS, heads * 2 * key_dim), keys.reshape(TOKENS, groups * 2 * key_dim))


def draw_queries_narrow(key, part):
    return pair_draw(key, HN, KN, DN, 11)[0].astype(jnp.bfloat16)


def draw_keys_narrow(key, part):
    return pair_draw(key, HN, KN, DN, 11)[1].astype(jnp.bfloat16)


def draw_queries_wide(key, part):
    return pair_draw(key, HW, KW, DW, 12)[0].astype(jnp.bfloat16)


def draw_keys_wide(key, part):
    return pair_draw(key, HW, KW, DW, 12)[1].astype(jnp.bfloat16)


def block_levels(rng, dims, pieces, low, high):
    gain, own = 1.0, jax.random.fold_in(rng, 6)
    for axis_at, shards_of in pieces:
        draws = jnp.exp(jax.random.uniform(jax.random.fold_in(own, axis_at), (shards_of,), jnp.float32, low / len(pieces), high / len(pieces)))
        gain = gain * jnp.repeat(draws, dims[axis_at] // shards_of).reshape([-1 if axis == axis_at else 1 for axis in range(len(dims))])
    return gain


def routed_block(rng, own, number, rows, amount, top, bound, slope):
    order = jax.random.permutation(rng, amount)
    crowded, usual = load_shares(amount, rows * top, bound, slope, True), load_shares(amount, rows * top, bound, slope, False)
    places = jnp.arange(amount)

    def named(tallies, rotation):
        used = int((tallies > 0).sum())
        fixed = max(1, used // 4)
        moved = fixed + (places - fixed + rotation * (used - fixed)) % max(1, amount - fixed)
        return jnp.zeros((amount,), jnp.int32).at[order[jnp.where(places < fixed, places, moved)]].set(jnp.asarray(tallies, jnp.int32))

    tallies = jnp.where(number % 4 == 0, named(crowded, number // 4), named(usual, number - number // 4 - 1))
    mixed = jax.random.permutation(jax.random.fold_in(own, 3), amount)
    source_of, sink = mixed[0:amount // 2 * 2:2], mixed[1:amount // 2 * 2:2]
    room = jnp.minimum(tallies[source_of] - 1, bound - tallies[sink]) // 2
    room = jnp.where((source_of == order[0]) | (sink == order[0]) | (tallies[sink] == 0), 0, jnp.maximum(room, 0))
    moved = jax.random.randint(jax.random.fold_in(own, 4), (amount // 2,), 0, 1 << 20) % (room + 1)
    tallies = tallies.at[source_of].add(-moved).at[sink].add(moved)
    items = jnp.searchsorted(jnp.cumsum(tallies), jnp.arange(rows * top), side="right").astype(jnp.int32)
    listing = items.reshape(top, rows).T
    listing = listing[jax.random.permutation(jax.random.fold_in(own, 1), rows)]
    rotation = jax.random.randint(jax.random.fold_in(own, 2), (rows, 1), 0, top)
    return jnp.take_along_axis(listing, (jnp.arange(top)[None, :] + rotation) % top, axis=1)


def load_shares(count, total, reach, lean, full):
    loads = [(1 << 20) // math.isqrt(rank ** lean) + 1 for rank in range(1, count + 1)]
    largest = reach if full else min(reach, max(-(-total // count), total * loads[0] // sum(loads)))
    least = 1 if total - largest >= count - 1 else 0
    given, rest = [largest] + [least] * (count - 1), total - largest - least * (count - 1)
    while rest > 0:
        movable = [i for i in range(1, count) if given[i] < largest] or [i for i in range(1, count) if given[i] < reach]
        whole, budget = sum([loads[i] for i in movable]), rest
        for i in movable:
            extra = min(reach - given[i], max(1, budget * loads[i] // whole), rest)
            given[i] = given[i] + extra
            rest = rest - extra
    return np.array(given)


def normal_values(key, extent, scale, limit, shards=(), kind=jnp.bfloat16):
    values = scale * jax.random.normal(key, extent, jnp.float32)
    if shards:
        values = values * block_levels(key, extent, shards, -0.22, 0.18)
    return jnp.clip(values, -limit, limit).astype(kind)


def setup_inputs(seed: int = 0) -> dict:
    key_list = jax.random.split(jax.random.key(seed), 25)
    queries_narrow = draw_queries_narrow(jax.random.fold_in(key_list[24], 71), 0)
    keys_narrow = draw_keys_narrow(jax.random.fold_in(key_list[24], 71), 0)
    values_narrow = normal_values(key_list[2], (TOKENS, KN * VN), 1.0, 6.0, ((0, 64), (1, 2)))
    queries_wide = draw_queries_wide(jax.random.fold_in(key_list[24], 71), 0)
    keys_wide = draw_keys_wide(jax.random.fold_in(key_list[24], 71), 0)
    values_wide = normal_values(key_list[5], (TOKENS, KW * VW), 1.0, 6.0, ((0, 64), (1, 2)))
    lambda_narrow = jnp.clip(0.3 + 0.5 * jax.random.uniform(key_list[6], (HN,), jnp.float32) ** block_levels(key_list[6], (HN,), ((0, 2),), -0.2, 0.2), 0.3, 0.8)
    lambda_wide = jnp.clip(0.3 + 0.5 * jax.random.uniform(key_list[7], (HW,), jnp.float32) ** block_levels(key_list[7], (HW,), ((0, 2),), -0.2, 0.2), 0.3, 0.8)
    gain_narrow = jnp.clip(1.0 + 0.18 * jax.random.normal(key_list[8], (VN,), jnp.float32), 0.1, 1.9)
    gain_wide = jnp.clip(1.0 + 0.18 * jax.random.normal(key_list[9], (VW,), jnp.float32), 0.1, 1.9)
    out_narrow = normal_values(key_list[10], (HN * VN, D), D ** -0.5, 0.125)
    out_wide = normal_values(key_list[11], (HW * VW, D), D ** -0.5, 0.125)
    stream = normal_values(key_list[12], (TOKENS, D), 1.0, 6.0, ((0, 128),))
    gain_mix = jnp.clip(1.0 + 0.18 * jax.random.normal(key_list[13], (D,), jnp.float32), 0.1, 1.9)
    gain_ffn = jnp.clip(1.0 + 0.18 * jax.random.normal(key_list[14], (D,), jnp.float32), 0.1, 1.9)
    gain_post = jnp.clip(1.0 + 0.18 * jax.random.normal(key_list[15], (D,), jnp.float32), 0.1, 1.9)
    shared_gate = normal_values(key_list[16], (D, SFF), D ** -0.5, 0.125)
    shared_up = normal_values(key_list[17], (D, SFF), D ** -0.5, 0.125)
    shared_down = normal_values(key_list[18], (SFF, D), SFF ** -0.5, 0.25)
    expert_gate = normal_values(key_list[19], (EXPERTS, D, FF), D ** -0.5, 0.125, ((0, 64), (2, 2)))
    expert_up = normal_values(key_list[20], (EXPERTS, D, FF), D ** -0.5, 0.125, ((0, 64), (2, 2)))
    expert_down = normal_values(key_list[21], (EXPERTS, FF, D), FF ** -0.5, 0.25, ((0, 64), (1, 2)))
    expert_ids_keys = jax.random.split(jax.random.fold_in(key_list[22], 1), TOKENS // (TOK_DEV // N_TP))
    expert_ids_turns = jax.random.permutation(jax.random.fold_in(key_list[22], 3), TOKENS // (TOK_DEV // N_TP))
    expert_ids = jax.vmap(lambda own, number: routed_block(jax.random.fold_in(key_list[22], 2), own, number, TOK_DEV // N_TP, EXPERTS, TOPK, CAP, 1))(expert_ids_keys, expert_ids_turns).reshape((TOKENS, TOPK))
    route_weights = jnp.clip(0.2 + 0.8 * jax.random.uniform(key_list[23], (TOKENS, TOPK), jnp.float32) ** block_levels(key_list[23], (TOKENS, TOPK), ((0, 128),), -0.2, 0.2), 0.2, 1.0)
    return {"queries_narrow": queries_narrow, "keys_narrow": keys_narrow, "values_narrow": values_narrow, "queries_wide": queries_wide, "keys_wide": keys_wide, "values_wide": values_wide, "lambda_narrow": lambda_narrow, "lambda_wide": lambda_wide, "gain_narrow": gain_narrow, "gain_wide": gain_wide, "out_narrow": out_narrow, "out_wide": out_wide, "stream": stream, "gain_mix": gain_mix, "gain_ffn": gain_ffn, "gain_post": gain_post, "shared_gate": shared_gate, "shared_up": shared_up, "shared_down": shared_down, "expert_gate": expert_gate, "expert_up": expert_up, "expert_down": expert_down, "expert_ids": expert_ids, "route_weights": route_weights}


EPS = 1e-06

def rms_scale(values, gain_row):
    return values * lax.rsqrt(lax.optimization_barrier(jnp.mean(values * values, axis=-1, keepdims=True)) + EPS) * gain_row

def round_trip(values):
    return lax.optimization_barrier(values.astype(jnp.bfloat16)).astype(jnp.float32)

def group_attention(queries, keys, values, lam_heads, gain_row, heads, groups, key_dim, value_dim):
    per_group = heads // groups
    length = queries.shape[0]
    blocks = length // TOK_DEV
    query_blocks = queries.reshape(blocks, TOK_DEV, groups, per_group, 2, key_dim)
    key_rows = keys.reshape(length, groups, 2, key_dim).astype(jnp.float32)
    value_rows = values.reshape(length, groups, value_dim).astype(jnp.float32)
    key_pos = jnp.arange(length, dtype=jnp.int32)
    lam_grid = lam_heads.reshape(groups, per_group)[:, :, None, None]

    def one_block(inputs):
        query_block, block_index = inputs
        query_pos = block_index * TOK_DEV + jnp.arange(TOK_DEV, dtype=jnp.int32)
        scores = jnp.einsum('qcgmd,kcmd->cgmqk', query_block.astype(jnp.float32), key_rows) * key_dim ** (-0.5)
        causal = key_pos[None, :] <= query_pos[:, None]
        scores = jnp.where(causal, scores, -1e+30)
        row_max = lax.optimization_barrier(jnp.max(scores, axis=-1, keepdims=True))
        weights = jnp.where(causal, jnp.exp(scores - row_max), 0.0)
        row_sum = lax.optimization_barrier(jnp.sum(weights, axis=-1))
        summed_values = jnp.einsum('cgmqk,kcv->cgmqv', round_trip(weights), value_rows)
        mapped = summed_values / row_sum[..., None]
        difference = mapped[:, :, 0] - lam_grid * mapped[:, :, 1]
        normed = rms_scale(difference, gain_row)
        return normed.transpose(2, 0, 1, 3).reshape(TOK_DEV, heads * value_dim).astype(jnp.bfloat16)
    outputs = lax.map(one_block, (query_blocks, jnp.arange(blocks, dtype=jnp.int32)))
    return outputs.reshape(length, heads * value_dim)

def routed_sum(normed, expert_gate, expert_up, expert_down, expert_ids, route_weights):
    assignments = TOKENS * TOPK
    flat_ids = expert_ids.reshape(-1)
    flat_weights = jnp.concatenate([route_weights.reshape(-1), jnp.zeros((1,), jnp.float32)])
    padded = jnp.concatenate([normed, jnp.zeros((1, D), jnp.bfloat16)], axis=0)
    row_bound = N_SP * N_TP * CAP
    half_width = FF // N_TP

    def per_expert(carried, expert):
        matches = jnp.nonzero(flat_ids == expert, size=row_bound, fill_value=assignments)[0].astype(jnp.int32)
        tokens_hit = matches // TOPK
        rows_in = padded[tokens_hit]
        gate_all = lax.dynamic_index_in_dim(expert_gate, expert, 0, keepdims=False)
        up_all = lax.dynamic_index_in_dim(expert_up, expert, 0, keepdims=False)
        down_all = lax.dynamic_index_in_dim(expert_down, expert, 0, keepdims=False)
        summed = jnp.zeros((row_bound, D), jnp.float32)
        for part_index in range(N_TP):
            low = part_index * half_width
            gate_cols = gate_all[:, low:low + half_width]
            up_cols = up_all[:, low:low + half_width]
            down_rows = down_all[low:low + half_width]
            hidden = (jax.nn.silu(jnp.dot(rows_in, gate_cols, preferred_element_type=jnp.float32)) * jnp.dot(rows_in, up_cols, preferred_element_type=jnp.float32)).astype(jnp.bfloat16)
            summed = summed + round_trip(jnp.dot(hidden, down_rows, preferred_element_type=jnp.float32))
        expert_out = round_trip(summed)
        weighted = expert_out * flat_weights[matches][:, None]
        return (carried.at[tokens_hit].add(weighted, mode='drop'), None)
    routed, unused = lax.scan(per_expert, jnp.zeros((TOKENS, D), jnp.float32), jnp.arange(EXPERTS, dtype=jnp.int32))
    return routed

def reference(queries_narrow, keys_narrow, values_narrow, queries_wide, keys_wide, values_wide, lambda_narrow, lambda_wide, gain_narrow, gain_wide, out_narrow, out_wide, stream, gain_mix, gain_ffn, gain_post, shared_gate, shared_up, shared_down, expert_gate, expert_up, expert_down, expert_ids, route_weights):
    narrow = group_attention(queries_narrow, keys_narrow, values_narrow, lambda_narrow, gain_narrow, HN, KN, DN, VN)
    wide = group_attention(queries_wide, keys_wide, values_wide, lambda_wide, gain_wide, HW, KW, DW, VW)
    projected = jnp.dot(narrow, out_narrow, preferred_element_type=jnp.float32) + jnp.dot(wide, out_wide, preferred_element_type=jnp.float32)
    mixed_rows = (stream.astype(jnp.float32) + rms_scale(projected, gain_mix)).astype(jnp.bfloat16)
    normed = rms_scale(mixed_rows.astype(jnp.float32), gain_ffn).astype(jnp.bfloat16)
    shared_hidden = (jax.nn.silu(jnp.dot(normed, shared_gate, preferred_element_type=jnp.float32)) * jnp.dot(normed, shared_up, preferred_element_type=jnp.float32)).astype(jnp.bfloat16)
    shared_out = jnp.dot(shared_hidden, shared_down, preferred_element_type=jnp.float32)
    routed = routed_sum(normed, expert_gate, expert_up, expert_down, expert_ids, route_weights)
    combined = shared_out + routed
    return (mixed_rows.astype(jnp.float32) + rms_scale(combined, gain_post)).astype(jnp.bfloat16)
```

```python
import functools

import jax
import jax.numpy as jnp
import numpy as np
from jax import lax
from jax.experimental import pallas as pl
from jax.experimental.pallas import tpu as pltpu
from jax.sharding import PartitionSpec as P

D = 2048
TOPK = 4
EPS = 1e-06
TQ = 128
LOG2E = 1.4426950408889634
BK = 1024
RC = 256
CAP = 6
PIECES = 4
WIDTH = D // PIECES
SLAB = PIECES * CAP
EXPERTS = 128
GROUP = 16
GROUP_ROWS = GROUP * SLAB
VMEM_BYTES = 60 * 2**20
MESH = pl.DeviceIdType.MESH
ORDERS = ((0, 1, 2), (1, 2, 0), (2, 0, 1))
STRIDE = (1, 4, 16)

def gather_kernel(kv, out, lsem, ssem, rsem):
    sp = lax.axis_index("sp")
    tp = lax.axis_index("tp")
    at = (sp % 4, (sp // 4) % 4, sp // 16)

    def moved(d, by):
        return sp + ((at[d] + by) % 4 - at[d]) * STRIDE[d]

    def dev(d, by):
        return (moved(d, by), tp)

    barrier = pltpu.get_barrier_semaphore()
    for d in range(3):
        for by in (1, 3):
            pl.semaphore_signal(barrier, inc=1, device_id=dev(d, by), device_id_type=MESH)
    pl.semaphore_wait(barrier, 6)
    own = pltpu.make_async_copy(kv, out.at[at[2], at[1], at[0]], lsem)
    own.start()

    def region(c, p, shift, lo, n):
        order = ORDERS[c]
        idx = [at[0], at[1], at[2]]
        for d in order[:p]:
            idx[d] = slice(None)
        idx[order[p]] = (at[order[p]] + shift) % 4
        return out.at[idx[2], idx[1], idx[0], pl.ds(lo, n), pl.ds(256 * c, 256)]

    def send(c, p, k, src, dst, by):
        s = (c * 3 + p) * 4 + k
        return pltpu.make_async_remote_copy(src_ref=src, dst_ref=dst, send_sem=ssem.at[s], recv_sem=rsem.at[s],
                                            device_id=dev(ORDERS[c][p], by), device_id_type=MESH)
    sends = []
    for p in range(3):
        first = []
        for c in range(3):
            dst = region(c, p, 0, 0, 256)
            src = kv.at[:, pl.ds(256 * c, 256)] if p == 0 else dst
            a = send(c, p, 0, src, dst, 1)
            b = send(c, p, 1, src, dst, 3)
            a.start(); b.start()
            first.append((a, b))
        second = []
        for c in range(3):
            a, b = first[c]
            a.wait_recv()
            r = region(c, p, 3, 0, 128)
            fa = send(c, p, 2, r, r, 1)
            fa.start()
            b.wait_recv()
            r = region(c, p, 1, 128, 128)
            fb = send(c, p, 3, r, r, 3)
            fb.start()
            second.append((fa, fb))
        if p == 0:
            own.wait()
        for c in range(3):
            for f in second[c]:
                f.wait_recv()
        sends += first + second
    for a, b in sends:
        a.wait_send()
        b.wait_send()

def gather(kv):
    return pl.pallas_call(
        gather_kernel,
        in_specs=[pl.BlockSpec(memory_space=pltpu.VMEM)],
        out_specs=pl.BlockSpec(memory_space=pl.ANY),
        out_shape=jax.ShapeDtypeStruct((4, 4, 4, 256, 768), jnp.bfloat16),
        scratch_shapes=[pltpu.SemaphoreType.DMA, pltpu.SemaphoreType.DMA((36,)), pltpu.SemaphoreType.DMA((36,))],
        compiler_params=pltpu.CompilerParams(collective_id=3, has_side_effects=True),
        name="gather",
    )(kv)


def flash_kernel(sched, q_ref, kv_ref, lamn_ref, lamw_ref, gn_ref, gw_ref, o_ref, qn, qw, mn, mw, accn, accw, lw):
    s = pl.program_id(0)
    n_hi = sched[0]
    tile = (s >= n_hi).astype(jnp.int32)
    kb = s - tile * n_hi
    last = sched[0] * (1 - tile) + sched[1] * tile - 1
    base = sched[2 + tile]
    key0 = kb * BK

    @pl.when(kb == 0)
    def _():
        lane = lax.broadcasted_iota(jnp.int32, (TQ, 128), 1)
        z = jnp.zeros((TQ, 128), jnp.bfloat16)
        for h in range(4):
            qh = q_ref[0, :, h * 128:(h + 1) * 128]
            qn[h * TQ:(h + 1) * TQ, :] = jnp.where(lane < 64, qh, z)
            qn[(4 + h) * TQ:(5 + h) * TQ, :] = jnp.where(lane < 64, z, qh)
        for h in range(2):
            b = 512 + h * 256
            qw[h * TQ:(h + 1) * TQ, 0:128] = q_ref[0, :, b:b + 128]
            qw[h * TQ:(h + 1) * TQ, 128:256] = z
            qw[(2 + h) * TQ:(3 + h) * TQ, 0:128] = z
            qw[(2 + h) * TQ:(3 + h) * TQ, 128:256] = q_ref[0, :, b + 128:b + 256]
        mn[...] = jnp.full(mn.shape, -1e30, jnp.float32)
        mw[...] = jnp.full(mw.shape, -1e30, jnp.float32)
        accn[...] = jnp.zeros(accn.shape, jnp.float32)
        accw[...] = jnp.zeros(accw.shape, jnp.float32)
        lw[...] = jnp.zeros(lw.shape, jnp.float32)

    def step(masked):
        kn = kv_ref[:, 0:128]
        vn = jnp.concatenate([kv_ref[:, 128:256], jnp.ones((BK, 128), jnp.bfloat16)], axis=1)
        kw = kv_ref[:, 256:512]
        vw = kv_ref[:, 512:768]
        dn = (((1,), (1,)), ((), ()))
        chunks = [("n", r) for r in range(0, 8 * TQ, RC)] + [("w", r) for r in range(0, 4 * TQ, RC)]
        if masked:
            row = lax.broadcasted_iota(jnp.int32, (RC, BK), 0) & (TQ - 1)
            col = lax.broadcasted_iota(jnp.int32, (RC, BK), 1)
            keep = (col + key0) <= (row + base)

        def scores(c):
            kind, r = c
            if kind == "n":
                return lax.dot_general(qn[r:r + RC, :], kn, dn, preferred_element_type=jnp.float32)
            return lax.dot_general(qw[r:r + RC, :], kw, dn, preferred_element_type=jnp.float32)

        nxt = scores(chunks[0])
        for ci, c in enumerate(chunks):
            sc = nxt
            if ci + 1 < len(chunks):
                nxt = scores(chunks[ci + 1])
            kind, r = c
            m_ref = mn if kind == "n" else mw
            scale = (64 if kind == "n" else 128) ** -0.5 * LOG2E
            sc = sc * scale
            if masked:
                sc = jnp.where(keep, sc, -1e30)
            m_old = m_ref[r:r + RC, :]
            m_new = jnp.maximum(m_old, jnp.max(sc, axis=-1, keepdims=True))
            m_ref[r:r + RC, :] = m_new
            alpha = jnp.exp2(m_old - m_new)
            p = jnp.exp2(sc - jnp.tile(m_new, (1, BK // 128)))
            pb = p.astype(jnp.bfloat16)
            a2 = jnp.tile(alpha, (1, 2))
            if kind == "n":
                accn[r:r + RC, :] = accn[r:r + RC, :] * a2 + jnp.dot(pb, vn, preferred_element_type=jnp.float32)
            else:
                ps = p[:, 0:128]
                for j in range(1, BK // 128):
                    ps = ps + p[:, j * 128:(j + 1) * 128]
                lw[r:r + RC, :] = lw[r:r + RC, :] * alpha + ps
                accw[r:r + RC, :] = accw[r:r + RC, :] * a2 + jnp.dot(pb, vw, preferred_element_type=jnp.float32)

    @pl.when(kb < last)
    def _():
        step(False)

    @pl.when(kb == last)
    def _():
        step(True)
        for h in range(4):
            r0, r1 = h * TQ, (4 + h) * TQ
            d = accn[r0:r0 + TQ, 0:128] / accn[r0:r0 + TQ, 128:256] - lamn_ref[h] * (accn[r1:r1 + TQ, 0:128] / accn[r1:r1 + TQ, 128:256])
            d = d * lax.rsqrt(jnp.mean(d * d, axis=-1, keepdims=True) + EPS) * gn_ref[...]
            o_ref[0, :, h * 128:(h + 1) * 128] = d.astype(jnp.bfloat16)
        for h in range(2):
            r0, r1 = h * TQ, (2 + h) * TQ
            l0 = jnp.sum(lw[r0:r0 + TQ, :], axis=-1, keepdims=True)
            l1 = jnp.sum(lw[r1:r1 + TQ, :], axis=-1, keepdims=True)
            d = accw[r0:r0 + TQ, :] / l0 - lamw_ref[h] * (accw[r1:r1 + TQ, :] / l1)
            d = d * lax.rsqrt(jnp.mean(d * d, axis=-1, keepdims=True) + EPS) * gw_ref[...]
            o_ref[0, :, 512 + h * 256:512 + (h + 1) * 256] = d.astype(jnp.bfloat16)


def flash(sched, q, kv, lamn, lamw, gn, gw):
    steps = (kv.shape[0] // 256 + BK // 256) // (BK // 256)
    def tile_of(s, sc):
        return (s >= sc[0]).astype(jnp.int32)
    gs = pltpu.PrefetchScalarGridSpec(
        num_scalar_prefetch=1, grid=(steps,),
        in_specs=[
            pl.BlockSpec((1, TQ, 1024), lambda s, sc: (tile_of(s, sc), 0, 0)),
            pl.BlockSpec((BK, 768), lambda s, sc: (s - tile_of(s, sc) * sc[0], 0)),
            pl.BlockSpec(memory_space=pltpu.SMEM),
            pl.BlockSpec(memory_space=pltpu.SMEM),
            pl.BlockSpec((1, 128), lambda s, sc: (0, 0)),
            pl.BlockSpec((1, 256), lambda s, sc: (0, 0)),
        ],
        out_specs=pl.BlockSpec((1, TQ, 1024), lambda s, sc: (tile_of(s, sc), 0, 0)),
        scratch_shapes=[
            pltpu.VMEM((8 * TQ, 128), jnp.bfloat16), pltpu.VMEM((4 * TQ, 256), jnp.bfloat16),
            pltpu.VMEM((8 * TQ, 128), jnp.float32), pltpu.VMEM((4 * TQ, 128), jnp.float32),
            pltpu.VMEM((8 * TQ, 256), jnp.float32), pltpu.VMEM((4 * TQ, 256), jnp.float32),
            pltpu.VMEM((4 * TQ, 128), jnp.float32),
        ])
    return pl.pallas_call(
        flash_kernel, grid_spec=gs,
        out_shape=jax.ShapeDtypeStruct((2, TQ, 1024), jnp.bfloat16),
        compiler_params=pltpu.CompilerParams(dimension_semantics=("arbitrary",), vmem_limit_bytes=VMEM_BYTES),
        name="flash",
    )(sched, q, kv, lamn, lamw, gn.reshape(1, 128), gw.reshape(1, 256))

def sched_of(i, n_blocks):
    a = jnp.minimum(i, n_blocks - 1 - i); b = n_blocks - 1 - a
    h = (i >= n_blocks // 2).astype(jnp.int32)
    w = BK // 256
    return jnp.stack([(b + w) // w, (a + w) // w, b * 256 + h * 128, a * 256 + h * 128]).astype(jnp.int32)


def rms(v, gain):
    return v * lax.rsqrt(jnp.mean(v * v, axis=-1, keepdims=True) + EPS) * gain


def dot(a, b):
    return jnp.dot(a, b, preferred_element_type=jnp.float32)


def ranks(ids):
    lane = lax.broadcasted_iota(jnp.int32, (TQ, EXPERTS), 1)
    named = jnp.zeros((TQ, EXPERTS), jnp.float32)
    for k in range(TOPK):
        named = named + (ids[:, k : k + 1] == lane).astype(jnp.float32)
    below = lax.broadcasted_iota(jnp.int32, (TQ, TQ), 1) < lax.broadcasted_iota(
        jnp.int32, (TQ, TQ), 0
    )
    count = dot(below.astype(jnp.bfloat16), named.astype(jnp.bfloat16))
    return (named * (count + 1.0)).astype(jnp.bfloat16)


def mid_kernel(
    f0, f1, on, ow, stream, gmix, gffn, ids, rank_of, piece_mask, mixed_out, normed_out, slab
):
    projected = (
        dot(f0[:, 0:512], on[0:512, :])
        + dot(f1[:, 0:512], on[512:1024, :])
        + dot(f0[:, 512:1024], ow[0:512, :])
        + dot(f1[:, 512:1024], ow[512:1024, :])
    )
    mixed = (stream[...].astype(jnp.float32) + rms(projected, gmix[...])).astype(jnp.bfloat16)
    mixed_out[...] = mixed
    normed = rms(mixed.astype(jnp.float32), gffn[...]).astype(jnp.bfloat16)
    normed_out[...] = normed
    stacked = jnp.concatenate([normed[:, c * WIDTH : (c + 1) * WIDTH] for c in range(PIECES)], 0)
    value = ranks(ids[...])
    row = lax.broadcasted_iota(jnp.int32, (GROUP_ROWS, EXPERTS), 0)
    lane = lax.broadcasted_iota(jnp.int32, (GROUP_ROWS, EXPERTS), 1)
    for g in range(EXPERTS // GROUP):
        low = (lane - g * GROUP) * SLAB
        spread = ((row >= low) & (row < low + SLAB)).astype(jnp.bfloat16)
        here = lax.dot_general(
            spread, value, (((1,), (1,)), ((), ())), preferred_element_type=jnp.float32
        )
        chosen = (here == rank_of[...]).astype(jnp.float32).astype(jnp.bfloat16)
        chosen = jnp.concatenate([chosen] * PIECES, axis=1) * piece_mask[...]
        slab[g * GROUP_ROWS : (g + 1) * GROUP_ROWS, :] = dot(chosen, stacked).astype(jnp.bfloat16)


def slab_tables():
    i = np.arange(GROUP_ROWS) % SLAB
    rank = np.broadcast_to((i % CAP + 1)[:, None], (GROUP_ROWS, EXPERTS)).astype(np.float32)
    piece = (i // CAP)[:, None] == (np.arange(PIECES * TQ) // TQ)[None, :]
    return rank, piece.astype(np.float32)


def order_table():
    i = np.arange(GROUP_ROWS)
    to = (i % SLAB // CAP) * (GROUP * CAP) + (i // SLAB) * CAP + i % CAP
    table = np.zeros((GROUP_ROWS, GROUP_ROWS), np.float32)
    table[to, i] = 1.0
    return table


def mid(f0, f1, on, ow, stream, gmix, gffn, ids):
    rank, piece = slab_tables()
    return pl.pallas_call(
        mid_kernel,
        out_shape=(
            jax.ShapeDtypeStruct((TQ, D), jnp.bfloat16),
            jax.ShapeDtypeStruct((TQ, D), jnp.bfloat16),
            jax.ShapeDtypeStruct((EXPERTS * SLAB, WIDTH), jnp.bfloat16),
        ),
        compiler_params=pltpu.CompilerParams(vmem_limit_bytes=VMEM_BYTES),
        cost_estimate=pl.CostEstimate(flops=4 * 10**9, bytes_accessed=14 * 10**6, transcendentals=0),
        name="mid",
    )(
        f0,
        f1,
        on,
        ow,
        stream,
        gmix.reshape(1, D),
        gffn.reshape(1, D),
        ids,
        jnp.asarray(rank),
        jnp.asarray(piece, jnp.bfloat16),
    )


def expert_kernel(x, g1, u1, d1, g2, u2, d2, order, order_t, out, rows, results):
    span = GROUP * CAP
    for g in range(EXPERTS // GROUP):
        got = dot(order[...], x[g * GROUP_ROWS : (g + 1) * GROUP_ROWS, :]).astype(jnp.bfloat16)
        for c in range(PIECES):
            rows[g * span : (g + 1) * span, c * WIDTH : (c + 1) * WIDTH] = got[
                c * span : (c + 1) * span, :
            ]
    for m in range(0, EXPERTS * CAP, 256):
        part = rows[m : m + 256, :]
        total = None
        for gate, up, down in ((g1, u1, d1), (g2, u2, d2)):
            gated = dot(part, gate[0])
            hidden = (gated / (1.0 + jnp.exp(-gated)) * dot(part, up[0])).astype(jnp.bfloat16)
            term = dot(hidden, down[0])
            total = term if total is None else total + term
        results[m : m + 256, :] = total.astype(jnp.bfloat16)
    for g in range(EXPERTS // GROUP):
        stacked = jnp.concatenate(
            [
                results[g * span : (g + 1) * span, c * WIDTH : (c + 1) * WIDTH]
                for c in range(PIECES)
            ],
            0,
        )
        out[g * GROUP_ROWS : (g + 1) * GROUP_ROWS, :] = dot(order_t[...], stacked).astype(
            jnp.bfloat16
        )


def run_expert(which, x, gate, up, down, gate2, up2, down2):
    table = order_table()
    full = lambda *shape: pl.BlockSpec(shape, lambda i, w: (0,) * len(shape))
    mine = lambda *shape: pl.BlockSpec((1, *shape), lambda i, w: (w[0], 0, 0))
    half = gate.shape[2]
    return pl.pallas_call(
        expert_kernel_with_prefetch,
        grid_spec=pltpu.PrefetchScalarGridSpec(
            num_scalar_prefetch=1,
            grid=(1,),
            in_specs=[
                full(EXPERTS * SLAB, WIDTH),
                mine(D, half),
                mine(D, half),
                mine(half, D),
                full(1, D, half),
                full(1, D, half),
                full(1, half, D),
                full(GROUP_ROWS, GROUP_ROWS),
                full(GROUP_ROWS, GROUP_ROWS),
            ],
            out_specs=full(EXPERTS * SLAB, WIDTH),
            scratch_shapes=[
                pltpu.VMEM((EXPERTS * CAP, D), jnp.bfloat16),
                pltpu.VMEM((EXPERTS * CAP, D), jnp.bfloat16),
            ],
        ),
        out_shape=jax.ShapeDtypeStruct((EXPERTS * SLAB, WIDTH), jnp.bfloat16),
        compiler_params=pltpu.CompilerParams(vmem_limit_bytes=VMEM_BYTES),
        cost_estimate=pl.CostEstimate(flops=6 * 10**9, bytes_accessed=14 * 10**6, transcendentals=0),
        name="expert",
    )(
        which,
        x,
        gate,
        up,
        down,
        gate2,
        up2,
        down2,
        jnp.asarray(table, jnp.bfloat16),
        jnp.asarray(table.T, jnp.bfloat16),
    )


def expert_kernel_with_prefetch(which, *refs):
    expert_kernel(*refs)


def combine_kernel(back, ids, weights, shared, mixed, gpost, rank_row, piece_row, out):
    value = ranks(ids[...])
    lane = lax.broadcasted_iota(jnp.int32, (TQ, EXPERTS), 1)
    share = jnp.zeros((TQ, EXPERTS), jnp.float32)
    for k in range(TOPK):
        share = share + jnp.where(ids[:, k : k + 1] == lane, weights[:, k : k + 1], 0.0)
    share = share.astype(jnp.bfloat16)
    row = lax.broadcasted_iota(jnp.int32, (EXPERTS, GROUP_ROWS), 0)
    col = lax.broadcasted_iota(jnp.int32, (EXPERTS, GROUP_ROWS), 1)
    total = jnp.zeros((PIECES * TQ, WIDTH), jnp.float32)
    for g in range(EXPERTS // GROUP):
        low = (row - g * GROUP) * SLAB
        spread = ((col >= low) & (col < low + SLAB)).astype(jnp.bfloat16)
        held = jnp.where(dot(value, spread) == rank_row[...], dot(share, spread), 0.0)
        picks = jnp.concatenate(
            [jnp.where(piece_row[...] == float(c), held, 0.0) for c in range(PIECES)], 0
        ).astype(jnp.bfloat16)
        total = total + dot(picks, back[g * GROUP_ROWS : (g + 1) * GROUP_ROWS, :])
    routed = jnp.concatenate([total[c * TQ : (c + 1) * TQ, :] for c in range(PIECES)], axis=1)
    combined = shared[...] + routed
    out[...] = (mixed[...].astype(jnp.float32) + rms(combined, gpost[...])).astype(jnp.bfloat16)


def combine(back, ids, weights, shared, mixed, gpost):
    i = np.arange(GROUP_ROWS) % SLAB
    return pl.pallas_call(
        combine_kernel,
        out_shape=jax.ShapeDtypeStruct((TQ, D), jnp.bfloat16),
        compiler_params=pltpu.CompilerParams(vmem_limit_bytes=VMEM_BYTES),
        cost_estimate=pl.CostEstimate(flops=3 * 10**9, bytes_accessed=6 * 10**6, transcendentals=0),
        name="combine",
    )(
        back,
        ids,
        weights,
        shared,
        mixed,
        gpost.reshape(1, D),
        jnp.asarray((i % CAP + 1)[None, :], jnp.float32),
        jnp.asarray((i // CAP)[None, :], jnp.float32),
    )


BOTH = ("sp", "tp")


def exchanged(slab):
    pieces = slab.reshape(EXPERTS, SLAB, WIDTH)
    return lax.all_to_all(pieces, BOTH, 0, 0, tiled=True).reshape(EXPERTS * SLAB, WIDTH)


def shards(
    queries_narrow,
    keys_narrow,
    values_narrow,
    queries_wide,
    keys_wide,
    values_wide,
    lambda_narrow,
    lambda_wide,
    gain_narrow,
    gain_wide,
    out_narrow,
    out_wide,
    stream,
    gain_mix,
    gain_ffn,
    gain_post,
    shared_gate,
    shared_up,
    shared_down,
    expert_gate,
    expert_up,
    expert_down,
    expert_ids,
    route_weights,
):
    sp = lax.axis_index("sp")
    tp = lax.axis_index("tp")
    n_sp = lax.axis_size("sp")
    late = sp >= n_sp // 2
    half = late.astype(jnp.int32)

    kv = jnp.concatenate([keys_narrow, values_narrow, keys_wide, values_wide], axis=1)
    queries = jnp.concatenate([queries_narrow, queries_wide], axis=1)
    mirror = [(i, n_sp - 1 - i) for i in range(n_sp)]
    kept = lax.dynamic_slice_in_dim(queries, half * TQ, TQ, 0)
    given = lax.dynamic_slice_in_dim(queries, (1 - half) * TQ, TQ, 0)
    taken = lax.ppermute(given, "sp", mirror)
    tiles = jnp.stack([jnp.where(late, kept, taken), jnp.where(late, taken, kept)])
    across = [(0, 1), (1, 0)]
    other = [
        lax.ppermute(lax.dynamic_slice_in_dim(w, 1 - tp, 1, 0), "tp", across)
        for w in (expert_gate, expert_up, expert_down)
    ]
    gathered = gather(kv).reshape(n_sp * 2 * TQ, kv.shape[1])
    attended = flash(
        sched_of(sp, n_sp), tiles, gathered, lambda_narrow, lambda_wide, gain_narrow, gain_wide
    )
    own = jnp.where(late, attended[0], attended[1])
    away = jnp.where(late, attended[1], attended[0])
    first, second = [], []
    for i in range(n_sp):
        h = int(i >= n_sp // 2)
        home, abroad = 2 * i + h, 2 * (n_sp - 1 - i) + h
        first += [(2 * i, home), (2 * i + 1, abroad)]
        second += [(2 * i, abroad), (2 * i + 1, home)]
    a = lax.ppermute(jnp.where(tp == 0, own, away), BOTH, first)
    b = lax.ppermute(jnp.where(tp == 0, away, own), BOTH, second)
    f0 = jnp.where(tp == half, a, b)
    f1 = jnp.where(tp == half, b, a)
    mixed, normed, slab = mid(
        f0, f1, out_narrow, out_wide, stream, gain_mix, gain_ffn, expert_ids
    )
    incoming = exchanged(slab)
    results = run_expert(
        jnp.reshape(tp, (1,)).astype(jnp.int32),
        incoming,
        expert_gate,
        expert_up,
        expert_down,
        *other,
    )
    back = exchanged(results)
    shared_hidden = (
        jax.nn.silu(dot(normed, shared_gate)) * dot(normed, shared_up)
    ).astype(jnp.bfloat16)
    shared_out = dot(shared_hidden, shared_down)
    return combine(back, expert_ids, route_weights, shared_out, mixed, gain_post)


def solution(mesh):
    return jax.shard_map(
        shards,
        mesh=mesh,
        in_specs=(
            P("sp", "tp"),
            P("sp", "tp"),
            P("sp", "tp"),
            P("sp", "tp"),
            P("sp", "tp"),
            P("sp", "tp"),
            P("tp"),
            P("tp"),
            P(),
            P(),
            P(),
            P(),
            P(("sp", "tp"), None),
            P(),
            P(),
            P(),
            P(),
            P(),
            P(),
            P("sp", None, "tp"),
            P("sp", None, "tp"),
            P("sp", "tp", None),
            P(("sp", "tp"), None),
            P(("sp", "tp"), None),
        ),
        out_specs=P(("sp", "tp"), None),
        check_vma=False,
    )
```

```python
import functools

import jax
import jax.numpy as jnp
import numpy as np
from jax import lax
from jax.experimental import pallas as pl
from jax.experimental.pallas import tpu as pltpu
from jax.sharding import PartitionSpec as P

D = 2048
TOPK = 4
EPS = 1e-06
TQ = 128
LOG2E = 1.4426950408889634
RC = 256
CAP = 6
PIECES = 4
WIDTH = D // PIECES
SLAB = PIECES * CAP
EXPERTS = 128
GROUP = 16
GROUP_ROWS = GROUP * SLAB
ATTN_BYTES = 60 * 2**20
VMEM_BYTES = 60 * 2**20
MESH = pl.DeviceIdType.MESH
ORDERS = ((0, 1, 2), (1, 2, 0), (2, 0, 1))
STRIDE = (1, 4, 16)

CHUNKS = ((0, 64), (64, 64), (128, 64), (192, 32), (224, 32))
SPANS = (5, 5, 5, 3, 3)
STARTS = (0, 5, 10, 15, 18)
STEPS = 21
TURNS = {1: 2, 2: 7, 3: 11, 4: 14}
KEYS = 1024


def attn_kernel(
    qn_in, qw_in, kn_in, vn_in, kw_in, vw_in, lamn, lamw, gn, gw, relpos,
    kvall, out,
    kv, buf, qgot_n, qgot_w, qn, qw, mn, mw, accn, accw, lw, att, fin,
    isem, osem, qs, qr, ssem, rsem, bsem, ds, dr,
):
    sp = lax.axis_index("sp")
    tp = lax.axis_index("tp")
    half = sp // 32
    at = (sp % 4, (sp // 4) % 4, sp // 16)
    mirror = 63 - sp

    def dev(d, by):
        return (sp + ((at[d] + by) % 4 - at[d]) * STRIDE[d], tp)

    loads = []
    for i, (src, lo, n) in enumerate(
        ((kn_in, 0, 128), (vn_in, 128, 128), (kw_in, 256, 256), (vw_in, 512, 256))
    ):
        copy = pltpu.make_async_copy(src, kv.at[:, pl.ds(lo, n)], isem.at[i])
        copy.start()
        loads.append(copy)

    barrier = pltpu.get_barrier_semaphore()
    for d in range(3):
        for by in (1, 3):
            pl.semaphore_signal(barrier, inc=1, device_id=dev(d, by), device_id_type=MESH)
    for who in ((sp, 1 - tp), (mirror, tp), (mirror, 1 - tp)):
        pl.semaphore_signal(barrier, inc=1, device_id=who, device_id_type=MESH)
    pl.semaphore_wait(barrier, 9)
    for copy in loads:
        copy.wait()
    own = pltpu.make_async_copy(kv, kvall.at[at[2], at[1], at[0]], osem)
    own.start()

    def region(c, p, shift, lo, n):
        order = ORDERS[c]
        idx = [at[0], at[1], at[2]]
        for d in order[:p]:
            idx[d] = slice(None)
        idx[order[p]] = (at[order[p]] + shift) % 4
        return kvall.at[idx[2], idx[1], idx[0], pl.ds(lo, n), pl.ds(256 * c, 256)]

    def send(c, p, k, src, dst, by, chunk=0):
        s = (c * 7 + p + chunk) * 6 + k
        return pltpu.make_async_remote_copy(
            src_ref=src, dst_ref=dst, send_sem=ssem.at[s], recv_sem=rsem.at[s],
            device_id=dev(ORDERS[c][p], by), device_id_type=MESH,
        )

    def direct(c, p, lo, n, chunk, later):
        m = n // 2
        found = []
        for k, by in ((0, 1), (1, 3)):
            at_row = lo + m * ((k + later) % 2)
            dst = region(c, p, 0, at_row, m)
            src = kv.at[pl.ds(at_row, m), pl.ds(256 * c, 256)] if p == 0 else dst
            found.append(send(c, p, k + 2 * later, src, dst, by, chunk))
        return found

    def passed(c, p, lo, n, chunk):
        m = n // 2
        r1 = region(c, p, 3, lo, m)
        r2 = region(c, p, 1, lo + m, m)
        return send(c, p, 4, r1, r1, 1, chunk), send(c, p, 5, r2, r2, 3, chunk)

    def begin(p, lo=0, n=256, chunk=0):
        for later in range(2):
            for c in range(3):
                for x in direct(c, p, lo, n, chunk, later):
                    x.start()

    def middle(p, lo=0, n=256, chunk=0):
        for c in range(3):
            for x, y in zip(direct(c, p, lo, n, chunk, 0), passed(c, p, lo, n, chunk)):
                x.wait_recv()
                y.start()

    def end(p, lo=0, n=256, chunk=0):
        for c in range(3):
            for x in (*direct(c, p, lo, n, chunk, 1), *passed(c, p, lo, n, chunk)):
                x.wait_recv()

    def drain(p, lo=0, n=256, chunk=0):
        for c in range(3):
            for later in range(2):
                for x in direct(c, p, lo, n, chunk, later):
                    x.wait_send()
            for x in passed(c, p, lo, n, chunk):
                x.wait_send()

    def queries(k, src, dst):
        return pltpu.make_async_remote_copy(
            src_ref=src.at[pl.ds((1 - half) * TQ, TQ), :], dst_ref=dst, send_sem=qs.at[k],
            recv_sem=qr.at[k], device_id=(mirror, tp), device_id_type=MESH,
        )

    qcopies = (queries(0, qn_in, qgot_n), queries(1, qw_in, qgot_w))
    begin(0)
    middle(0)
    own.wait()
    end(0)
    begin(1)
    for x in qcopies:
        x.start()
    middle(1)
    end(1)
    begin(2, *CHUNKS[0], 0)

    for x in qcopies:
        x.wait_recv()
    lane = lax.broadcasted_iota(jnp.int32, (TQ, 128), 1)
    zero = jnp.zeros((TQ, 128), jnp.bfloat16)
    for mine in (1, 0):
        tile = 1 - half if mine else half
        for h in range(4):
            col = slice(h * 128, (h + 1) * 128)
            rows = qn_in[pl.ds(half * TQ, TQ), col] if mine else qgot_n[:, col]
            qn[tile, h * TQ : (h + 1) * TQ, :] = jnp.where(lane < 64, rows, zero)
            qn[tile, (4 + h) * TQ : (5 + h) * TQ, :] = jnp.where(lane < 64, zero, rows)
        for h in range(2):
            for m in range(2):
                col = slice(h * 256 + m * 128, h * 256 + (m + 1) * 128)
                rows = qw_in[pl.ds(half * TQ, TQ), col] if mine else qgot_w[:, col]
                put = slice((2 * m + h) * TQ, (2 * m + h + 1) * TQ)
                qw[tile, put, m * 128 : (m + 1) * 128] = rows
                qw[tile, put, (1 - m) * 128 : (2 - m) * 128] = zero
    mn[...] = jnp.full(mn.shape, -1e30, jnp.float32)
    mw[...] = jnp.full(mw.shape, -1e30, jnp.float32)
    accn[...] = jnp.zeros(accn.shape, jnp.float32)
    accw[...] = jnp.zeros(accw.shape, jnp.float32)
    lw[...] = jnp.zeros(lw.shape, jnp.float32)

    middle(2, *CHUNKS[0], 0)
    begin(2, *CHUNKS[1], 1)

    low = half * mirror + (1 - half) * sp
    high = 63 - low

    def place(s):
        after = [(s >= start).astype(jnp.int32) for start in STARTS]
        j = s - sum(SPANS[k - 1] * after[k] for k in range(1, len(CHUNKS)))
        width = 16 + 16 * after[3]
        n_hi = high // width + 1
        n_lo = low // width + 1
        turned = half * after[4]
        first = n_hi * (1 - turned) + n_lo * turned
        second = (j >= first).astype(jnp.int32)
        tile = turned + second - 2 * turned * second
        g = j - second * first
        last = n_hi * (1 - tile) + n_lo * tile - 1
        row = sum((CHUNKS[k][0] - CHUNKS[k - 1][0]) * after[k] for k in range(1, len(CHUNKS)))
        return after, row, tile, g, g == last, g * width * 256 + row

    def fetch(s, slot):
        after, row, _, g, _, _ = place(s)

        @pl.when(after[3] == 0)
        def _():
            for k in range(16):
                pltpu.make_async_copy(
                    kvall.at[g, k // 4, k % 4, pl.ds(pl.multiple_of(row, 32), 64), :],
                    buf.at[slot, k // 4, pl.ds((k % 4) * 64, 64), :], bsem.at[slot],
                ).start()

        @pl.when(after[3] == 1)
        def _():
            for k in range(32):
                pltpu.make_async_copy(
                    kvall.at[2 * g + k // 16, k // 4 % 4, k % 4, pl.ds(pl.multiple_of(row, 32), 32), :],
                    buf.at[slot, k // 8, pl.ds((k % 8) * 32, 32), :], bsem.at[slot],
                ).start()

    def finish(tile):
        for h in range(4):
            r0, r1 = h * TQ, (4 + h) * TQ
            d = accn[tile, r0 : r0 + TQ, 0:128] / accn[tile, r0 : r0 + TQ, 128:256] - lamn[h] * (
                accn[tile, r1 : r1 + TQ, 0:128] / accn[tile, r1 : r1 + TQ, 128:256]
            )
            d = d * lax.rsqrt(jnp.mean(d * d, axis=-1, keepdims=True) + EPS) * gn[...]
            att[tile, :, h * 128 : (h + 1) * 128] = d.astype(jnp.bfloat16)
        for h in range(2):
            r0, r1 = h * TQ, (2 + h) * TQ
            l0 = jnp.sum(lw[tile, r0 : r0 + TQ, :], axis=-1, keepdims=True)
            l1 = jnp.sum(lw[tile, r1 : r1 + TQ, :], axis=-1, keepdims=True)
            d = accw[tile, r0 : r0 + TQ, :] / l0 - lamw[h] * (accw[tile, r1 : r1 + TQ, :] / l1)
            d = d * lax.rsqrt(jnp.mean(d * d, axis=-1, keepdims=True) + EPS) * gw[...]
            att[tile, :, 512 + h * 256 : 512 + (h + 1) * 256] = d.astype(jnp.bfloat16)

    def deliver(k, tile, who):
        return pltpu.make_async_remote_copy(
            src_ref=att.at[tile], dst_ref=fin.at[tp], send_sem=ds.at[k], recv_sem=dr.at[tp],
            device_id=who, device_id_type=MESH,
        )

    def step(s, carry):
        slot = s % 2
        after, _, tile, g, masked, first_key = place(s)
        for chunk in range(len(CHUNKS)):
            @pl.when(s == STARTS[chunk])
            def _():
                end(2, *CHUNKS[chunk], chunk)
                fetch(s, slot)
        for chunk, turn in TURNS.items():
            @pl.when(s == turn)
            def _():
                middle(2, *CHUNKS[chunk], chunk)
                if chunk + 1 < len(CHUNKS):
                    begin(2, *CHUNKS[chunk + 1], chunk + 1)

        @pl.when(s == STEPS - 1 - half)
        def _():
            finish(half)
            deliver(0, half, (mirror, half)).start()

        pltpu.make_async_copy(kvall.at[0, 0], buf.at[slot], bsem.at[slot]).wait()

        more = s + 1 < STEPS
        for start in STARTS[1:]:
            more = more & (s + 1 != start)

        @pl.when(more)
        def _():
            fetch(s + 1, 1 - slot)

        base = half * TQ + (high * (1 - tile) + low * tile) * 256

        def attend(mask):
            def columns(lo, n):
                return buf[slot, :, :, lo : lo + n].reshape(KEYS, n)

            keys_n, keys_w, vals_w = columns(0, 128), columns(256, 256), columns(512, 256)
            vals_n = jnp.concatenate(
                [columns(128, 128), jnp.ones((KEYS, 128), jnp.bfloat16)], axis=1
            )
            dims = (((1,), (1,)), ((), ()))
            if mask:
                row = lax.broadcasted_iota(jnp.int32, (RC, KEYS), 0) % TQ
                keep = (relpos[after[3]] + first_key) <= (row + base)

            def scores(narrow, r):
                if narrow:
                    return lax.dot_general(
                        qn[tile, r : r + RC, :], keys_n, dims, preferred_element_type=jnp.float32
                    )
                return lax.dot_general(
                    qw[tile, r : r + RC, :], keys_w, dims, preferred_element_type=jnp.float32
                )

            parts = [(True, r) for r in range(0, 8 * TQ, RC)]
            parts += [(False, r) for r in range(0, 4 * TQ, RC)]
            following = scores(*parts[0])
            for i, (narrow, r) in enumerate(parts):
                sc = following
                if i + 1 < len(parts):
                    following = scores(*parts[i + 1])
                m_ref = mn if narrow else mw
                sc = sc * ((64 if narrow else 128) ** -0.5 * LOG2E)
                if mask:
                    sc = jnp.where(keep, sc, -1e30)
                m_old = m_ref[tile, r : r + RC, :]
                m_new = jnp.maximum(m_old, jnp.max(sc, axis=-1, keepdims=True))
                m_ref[tile, r : r + RC, :] = m_new
                alpha = jnp.exp2(m_old - m_new)
                p = jnp.exp2(sc - jnp.tile(m_new, (1, KEYS // 128)))
                pb = p.astype(jnp.bfloat16)
                twice = jnp.tile(alpha, (1, 2))
                if narrow:
                    accn[tile, r : r + RC, :] = accn[tile, r : r + RC, :] * twice + jnp.dot(
                        pb, vals_n, preferred_element_type=jnp.float32
                    )
                else:
                    ps = p[:, 0:128]
                    for j in range(1, KEYS // 128):
                        ps = ps + p[:, j * 128 : (j + 1) * 128]
                    lw[tile, r : r + RC, :] = lw[tile, r : r + RC, :] * alpha + ps
                    accw[tile, r : r + RC, :] = accw[tile, r : r + RC, :] * twice + jnp.dot(
                        pb, vals_w, preferred_element_type=jnp.float32
                    )

        @pl.when(jnp.logical_not(masked))
        def _():
            attend(False)

        @pl.when(masked)
        def _():
            attend(True)

        return carry

    lax.fori_loop(0, STEPS, step, 0)

    finish(1 - half)

    @pl.when(tp != half)
    def _():
        deliver(1, 1 - half, (sp, 1 - tp)).start()

    drain(0)
    drain(1)
    for chunk in range(len(CHUNKS)):
        drain(2, *CHUNKS[chunk], chunk)
    for x in qcopies:
        x.wait_send()

    def arrived(slot):
        pltpu.make_async_remote_copy(
            src_ref=att.at[0], dst_ref=fin.at[slot], send_sem=ds.at[0], recv_sem=dr.at[slot],
            device_id=(mirror, half), device_id_type=MESH,
        ).wait_recv()

    @pl.when(tp == half)
    def _():
        arrived(1 - tp)
        out[pl.ds(tp, 1)] = att[pl.ds(1 - half, 1)]
        out[pl.ds(1 - tp, 1)] = fin[pl.ds(1 - tp, 1)]

    @pl.when(tp != half)
    def _():
        arrived(0)
        arrived(1)
        out[...] = fin[...]
        deliver(1, 1 - half, (sp, 1 - tp)).wait_send()

    deliver(0, half, (mirror, half)).wait_send()


def attention(qn, qw, kn, vn, kw, vw, lamn, lamw, gn, gw):
    col = np.arange(KEYS)
    rel = np.stack([(col // n) * 256 + col % n for n in (64, 32)]).astype(np.int32)
    vmem = pl.BlockSpec(memory_space=pltpu.VMEM)
    smem = pl.BlockSpec(memory_space=pltpu.SMEM)
    hbm = pl.BlockSpec(memory_space=pltpu.HBM)
    f32, bf16 = jnp.float32, jnp.bfloat16
    dma = pltpu.SemaphoreType.DMA
    _, out = pl.pallas_call(
        attn_kernel,
        in_specs=[vmem, vmem, hbm, hbm, hbm, hbm, smem, smem, vmem, vmem, vmem],
        out_specs=(hbm, vmem),
        out_shape=(
            jax.ShapeDtypeStruct((4, 4, 4, 256, 768), bf16),
            jax.ShapeDtypeStruct((2, TQ, 1024), bf16),
        ),
        scratch_shapes=[
            pltpu.VMEM((256, 768), bf16),
            pltpu.VMEM((2, 4, 256, 768), bf16),
            pltpu.VMEM((TQ, 512), bf16),
            pltpu.VMEM((TQ, 512), bf16),
            pltpu.VMEM((2, 8 * TQ, 128), bf16),
            pltpu.VMEM((2, 4 * TQ, 256), bf16),
            pltpu.VMEM((2, 8 * TQ, 128), f32),
            pltpu.VMEM((2, 4 * TQ, 128), f32),
            pltpu.VMEM((2, 8 * TQ, 256), f32),
            pltpu.VMEM((2, 4 * TQ, 256), f32),
            pltpu.VMEM((2, 4 * TQ, 128), f32),
            pltpu.VMEM((2, TQ, 1024), bf16),
            pltpu.VMEM((2, TQ, 1024), bf16),
            dma((4,)),
            dma,
            dma((2,)),
            dma((2,)),
            dma((126,)),
            dma((126,)),
            dma((2,)),
            dma((2,)),
            dma((2,)),
        ],
        compiler_params=pltpu.CompilerParams(
            collective_id=3, has_side_effects=True, vmem_limit_bytes=ATTN_BYTES
        ),
        cost_estimate=pl.CostEstimate(
            flops=30 * 10**9, bytes_accessed=60 * 10**6, transcendentals=0
        ),
        name="attention",
    )(
        qn, qw, kn, vn, kw, vw, lamn, lamw, gn.reshape(1, 128), gw.reshape(1, 256),
        jnp.asarray(rel.reshape(2, 1, KEYS)),
    )
    return out


def rms(v, gain):
    return v * lax.rsqrt(jnp.mean(v * v, axis=-1, keepdims=True) + EPS) * gain


def dot(a, b):
    return jnp.dot(a, b, preferred_element_type=jnp.float32)


def ranks(ids):
    lane = lax.broadcasted_iota(jnp.int32, (TQ, EXPERTS), 1)
    named = jnp.zeros((TQ, EXPERTS), jnp.float32)
    for k in range(TOPK):
        named = named + (ids[:, k : k + 1] == lane).astype(jnp.float32)
    below = lax.broadcasted_iota(jnp.int32, (TQ, TQ), 1) < lax.broadcasted_iota(
        jnp.int32, (TQ, TQ), 0
    )
    count = dot(below.astype(jnp.bfloat16), named.astype(jnp.bfloat16))
    return (named * (count + 1.0)).astype(jnp.bfloat16)


def mid_kernel(
    f, on, ow, stream, gmix, gffn, ids, rank_of, piece_mask, mixed_out, normed_out, slab
):
    projected = (
        dot(f[0, :, 0:512], on[0:512, :])
        + dot(f[1, :, 0:512], on[512:1024, :])
        + dot(f[0, :, 512:1024], ow[0:512, :])
        + dot(f[1, :, 512:1024], ow[512:1024, :])
    )
    mixed = (stream[...].astype(jnp.float32) + rms(projected, gmix[...])).astype(jnp.bfloat16)
    mixed_out[...] = mixed
    normed = rms(mixed.astype(jnp.float32), gffn[...]).astype(jnp.bfloat16)
    normed_out[...] = normed
    stacked = jnp.concatenate([normed[:, c * WIDTH : (c + 1) * WIDTH] for c in range(PIECES)], 0)
    value = ranks(ids[...])
    row = lax.broadcasted_iota(jnp.int32, (GROUP_ROWS, EXPERTS), 0)
    lane = lax.broadcasted_iota(jnp.int32, (GROUP_ROWS, EXPERTS), 1)
    for g in range(EXPERTS // GROUP):
        low = (lane - g * GROUP) * SLAB
        spread = ((row >= low) & (row < low + SLAB)).astype(jnp.bfloat16)
        here = lax.dot_general(
            spread, value, (((1,), (1,)), ((), ())), preferred_element_type=jnp.float32
        )
        chosen = (here == rank_of[...]).astype(jnp.float32).astype(jnp.bfloat16)
        chosen = jnp.concatenate([chosen] * PIECES, axis=1) * piece_mask[...]
        slab[g * GROUP_ROWS : (g + 1) * GROUP_ROWS, :] = dot(chosen, stacked).astype(jnp.bfloat16)


def slab_tables():
    i = np.arange(GROUP_ROWS) % SLAB
    rank = np.broadcast_to((i % CAP + 1)[:, None], (GROUP_ROWS, EXPERTS)).astype(np.float32)
    piece = (i // CAP)[:, None] == (np.arange(PIECES * TQ) // TQ)[None, :]
    return rank, piece.astype(np.float32)


def order_table():
    i = np.arange(GROUP_ROWS)
    to = (i % SLAB // CAP) * (GROUP * CAP) + (i // SLAB) * CAP + i % CAP
    table = np.zeros((GROUP_ROWS, GROUP_ROWS), np.float32)
    table[to, i] = 1.0
    return table


def mid(f, on, ow, stream, gmix, gffn, ids):
    rank, piece = slab_tables()
    return pl.pallas_call(
        mid_kernel,
        out_shape=(
            jax.ShapeDtypeStruct((TQ, D), jnp.bfloat16),
            jax.ShapeDtypeStruct((TQ, D), jnp.bfloat16),
            jax.ShapeDtypeStruct((EXPERTS * SLAB, WIDTH), jnp.bfloat16),
        ),
        compiler_params=pltpu.CompilerParams(vmem_limit_bytes=VMEM_BYTES),
        cost_estimate=pl.CostEstimate(flops=4 * 10**9, bytes_accessed=14 * 10**6, transcendentals=0),
        name="mid",
    )(
        f,
        on,
        ow,
        stream,
        gmix.reshape(1, D),
        gffn.reshape(1, D),
        ids,
        jnp.asarray(rank),
        jnp.asarray(piece, jnp.bfloat16),
    )


def expert_kernel(x, g1, u1, d1, g2, u2, d2, order, order_t, out, rows, results):
    span = GROUP * CAP
    for g in range(EXPERTS // GROUP):
        got = dot(order[...], x[g * GROUP_ROWS : (g + 1) * GROUP_ROWS, :]).astype(jnp.bfloat16)
        for c in range(PIECES):
            rows[g * span : (g + 1) * span, c * WIDTH : (c + 1) * WIDTH] = got[
                c * span : (c + 1) * span, :
            ]
    for m in range(0, EXPERTS * CAP, 256):
        part = rows[m : m + 256, :]
        total = None
        for gate, up, down in ((g1, u1, d1), (g2, u2, d2)):
            gated = dot(part, gate[0])
            hidden = (gated / (1.0 + jnp.exp(-gated)) * dot(part, up[0])).astype(jnp.bfloat16)
            term = dot(hidden, down[0])
            total = term if total is None else total + term
        results[m : m + 256, :] = total.astype(jnp.bfloat16)
    for g in range(EXPERTS // GROUP):
        stacked = jnp.concatenate(
            [
                results[g * span : (g + 1) * span, c * WIDTH : (c + 1) * WIDTH]
                for c in range(PIECES)
            ],
            0,
        )
        out[g * GROUP_ROWS : (g + 1) * GROUP_ROWS, :] = dot(order_t[...], stacked).astype(
            jnp.bfloat16
        )


def run_expert(which, x, gate, up, down, gate2, up2, down2):
    table = order_table()
    full = lambda *shape: pl.BlockSpec(shape, lambda i, w: (0,) * len(shape))
    mine = lambda *shape: pl.BlockSpec((1, *shape), lambda i, w: (w[0], 0, 0))
    half = gate.shape[2]
    return pl.pallas_call(
        expert_kernel_with_prefetch,
        grid_spec=pltpu.PrefetchScalarGridSpec(
            num_scalar_prefetch=1,
            grid=(1,),
            in_specs=[
                full(EXPERTS * SLAB, WIDTH),
                mine(D, half),
                mine(D, half),
                mine(half, D),
                full(1, D, half),
                full(1, D, half),
                full(1, half, D),
                full(GROUP_ROWS, GROUP_ROWS),
                full(GROUP_ROWS, GROUP_ROWS),
            ],
            out_specs=full(EXPERTS * SLAB, WIDTH),
            scratch_shapes=[
                pltpu.VMEM((EXPERTS * CAP, D), jnp.bfloat16),
                pltpu.VMEM((EXPERTS * CAP, D), jnp.bfloat16),
            ],
        ),
        out_shape=jax.ShapeDtypeStruct((EXPERTS * SLAB, WIDTH), jnp.bfloat16),
        compiler_params=pltpu.CompilerParams(vmem_limit_bytes=VMEM_BYTES),
        cost_estimate=pl.CostEstimate(flops=6 * 10**9, bytes_accessed=14 * 10**6, transcendentals=0),
        name="expert",
    )(
        which,
        x,
        gate,
        up,
        down,
        gate2,
        up2,
        down2,
        jnp.asarray(table, jnp.bfloat16),
        jnp.asarray(table.T, jnp.bfloat16),
    )


def expert_kernel_with_prefetch(which, *refs):
    expert_kernel(*refs)


def combine_kernel(back, ids, weights, shared, mixed, gpost, rank_row, piece_row, out):
    value = ranks(ids[...])
    lane = lax.broadcasted_iota(jnp.int32, (TQ, EXPERTS), 1)
    share = jnp.zeros((TQ, EXPERTS), jnp.float32)
    for k in range(TOPK):
        share = share + jnp.where(ids[:, k : k + 1] == lane, weights[:, k : k + 1], 0.0)
    share = share.astype(jnp.bfloat16)
    row = lax.broadcasted_iota(jnp.int32, (EXPERTS, GROUP_ROWS), 0)
    col = lax.broadcasted_iota(jnp.int32, (EXPERTS, GROUP_ROWS), 1)
    total = jnp.zeros((PIECES * TQ, WIDTH), jnp.float32)
    for g in range(EXPERTS // GROUP):
        low = (row - g * GROUP) * SLAB
        spread = ((col >= low) & (col < low + SLAB)).astype(jnp.bfloat16)
        held = jnp.where(dot(value, spread) == rank_row[...], dot(share, spread), 0.0)
        picks = jnp.concatenate(
            [jnp.where(piece_row[...] == float(c), held, 0.0) for c in range(PIECES)], 0
        ).astype(jnp.bfloat16)
        total = total + dot(picks, back[g * GROUP_ROWS : (g + 1) * GROUP_ROWS, :])
    routed = jnp.concatenate([total[c * TQ : (c + 1) * TQ, :] for c in range(PIECES)], axis=1)
    combined = shared[...] + routed
    out[...] = (mixed[...].astype(jnp.float32) + rms(combined, gpost[...])).astype(jnp.bfloat16)


def combine(back, ids, weights, shared, mixed, gpost):
    i = np.arange(GROUP_ROWS) % SLAB
    return pl.pallas_call(
        combine_kernel,
        out_shape=jax.ShapeDtypeStruct((TQ, D), jnp.bfloat16),
        compiler_params=pltpu.CompilerParams(vmem_limit_bytes=VMEM_BYTES),
        cost_estimate=pl.CostEstimate(flops=3 * 10**9, bytes_accessed=6 * 10**6, transcendentals=0),
        name="combine",
    )(
        back,
        ids,
        weights,
        shared,
        mixed,
        gpost.reshape(1, D),
        jnp.asarray((i % CAP + 1)[None, :], jnp.float32),
        jnp.asarray((i // CAP)[None, :], jnp.float32),
    )


BOTH = ("sp", "tp")


def exchanged(slab):
    pieces = slab.reshape(EXPERTS, SLAB, WIDTH)
    return lax.all_to_all(pieces, BOTH, 0, 0, tiled=True).reshape(EXPERTS * SLAB, WIDTH)


def shards(
    queries_narrow,
    keys_narrow,
    values_narrow,
    queries_wide,
    keys_wide,
    values_wide,
    lambda_narrow,
    lambda_wide,
    gain_narrow,
    gain_wide,
    out_narrow,
    out_wide,
    stream,
    gain_mix,
    gain_ffn,
    gain_post,
    shared_gate,
    shared_up,
    shared_down,
    expert_gate,
    expert_up,
    expert_down,
    expert_ids,
    route_weights,
):
    tp = lax.axis_index("tp")
    across = [(0, 1), (1, 0)]
    other = [
        lax.ppermute(lax.dynamic_slice_in_dim(w, 1 - tp, 1, 0), "tp", across)
        for w in (expert_gate, expert_up, expert_down)
    ]
    attended = attention(
        queries_narrow,
        queries_wide,
        keys_narrow,
        values_narrow,
        keys_wide,
        values_wide,
        lambda_narrow,
        lambda_wide,
        gain_narrow,
        gain_wide,
    )
    mixed, normed, slab = mid(
        attended, out_narrow, out_wide, stream, gain_mix, gain_ffn, expert_ids
    )
    incoming = exchanged(slab)
    results = run_expert(
        jnp.reshape(tp, (1,)).astype(jnp.int32),
        incoming,
        expert_gate,
        expert_up,
        expert_down,
        *other,
    )
    back = exchanged(results)
    shared_hidden = (
        jax.nn.silu(dot(normed, shared_gate)) * dot(normed, shared_up)
    ).astype(jnp.bfloat16)
    shared_out = dot(shared_hidden, shared_down)
    return combine(back, expert_ids, route_weights, shared_out, mixed, gain_post)


def solution(mesh):
    return jax.shard_map(
        shards,
        mesh=mesh,
        in_specs=(
            P("sp", "tp"),
            P("sp", "tp"),
            P("sp", "tp"),
            P("sp", "tp"),
            P("sp", "tp"),
            P("sp", "tp"),
            P("tp"),
            P("tp"),
            P(),
            P(),
            P(),
            P(),
            P(("sp", "tp"), None),
            P(),
            P(),
            P(),
            P(),
            P(),
            P(),
            P("sp", None, "tp"),
            P("sp", None, "tp"),
            P("sp", "tp", None),
            P(("sp", "tp"), None),
            P(("sp", "tp"), None),
        ),
        out_specs=P(("sp", "tp"), None),
        check_vma=False,
    )
```

```python
import functools

import jax
import jax.numpy as jnp
import numpy as np
from jax import lax
from jax.experimental import pallas as pl
from jax.experimental.pallas import tpu as pltpu
from jax.sharding import PartitionSpec as P

D = 2048
TOPK = 4
EPS = 1e-06
TQ = 128
LOG2E = 1.4426950408889634
RC = 256
CAP = 6
PIECES = 4
WIDTH = D // PIECES
SLAB = PIECES * CAP
EXPERTS = 128
GROUP = 16
GROUP_ROWS = GROUP * SLAB
ATTN_BYTES = 60 * 2**20
VMEM_BYTES = 60 * 2**20
MESH = pl.DeviceIdType.MESH
VMEM = pl.BlockSpec(memory_space=pltpu.VMEM)
HBM = pl.BlockSpec(memory_space=pltpu.HBM)
ORDERS = ((0, 1, 2), (1, 2, 0), (2, 0, 1))
STRIDE = (1, 4, 16)

CHUNKS = ((0, 64), (64, 64), (128, 64), (192, 32), (224, 32))
SPANS = (5, 5, 5, 3, 3)
STARTS = (0, 5, 10, 15, 18)
STEPS = 21
TURNS = {1: 2, 2: 7, 3: 11, 4: 14}
KEYS = 1024


def attn_kernel(
    qn_in, qw_in, kn_in, vn_in, kw_in, vw_in, lamn, lamw, gn, gw, relpos,
    kvall, out,
    kv, buf, qgot_n, qgot_w, qn, qw, mn, mw, accn, accw, lw, att, fin,
    isem, osem, qs, qr, ssem, rsem, bsem, ds, dr,
):
    sp = lax.axis_index("sp")
    tp = lax.axis_index("tp")
    half = sp // 32
    at = (sp % 4, (sp // 4) % 4, sp // 16)
    mirror = 63 - sp

    def dev(d, by):
        return (sp + ((at[d] + by) % 4 - at[d]) * STRIDE[d], tp)

    loads = []
    for i, (src, lo, n) in enumerate(
        ((kn_in, 0, 128), (vn_in, 128, 128), (kw_in, 256, 256), (vw_in, 512, 256))
    ):
        copy = pltpu.make_async_copy(src, kv.at[:, pl.ds(lo, n)], isem.at[i])
        copy.start()
        loads.append(copy)

    barrier = pltpu.get_barrier_semaphore()
    for d in range(3):
        for by in (1, 3):
            pl.semaphore_signal(barrier, inc=1, device_id=dev(d, by), device_id_type=MESH)
    for who in ((sp, 1 - tp), (mirror, tp), (mirror, 1 - tp)):
        pl.semaphore_signal(barrier, inc=1, device_id=who, device_id_type=MESH)
    pl.semaphore_wait(barrier, 9)
    for copy in loads:
        copy.wait()
    own = pltpu.make_async_copy(kv, kvall.at[at[2], at[1], at[0]], osem)
    own.start()

    def region(c, p, shift, lo, n):
        order = ORDERS[c]
        idx = [at[0], at[1], at[2]]
        for d in order[:p]:
            idx[d] = slice(None)
        idx[order[p]] = (at[order[p]] + shift) % 4
        return kvall.at[idx[2], idx[1], idx[0], pl.ds(lo, n), pl.ds(256 * c, 256)]

    def send(c, p, k, src, dst, by, chunk=0):
        s = (c * 7 + p + chunk) * 6 + k
        return pltpu.make_async_remote_copy(
            src_ref=src, dst_ref=dst, send_sem=ssem.at[s], recv_sem=rsem.at[s],
            device_id=dev(ORDERS[c][p], by), device_id_type=MESH,
        )

    def direct(c, p, lo, n, chunk, later):
        m = n // 2
        found = []
        for k, by in ((0, 1), (1, 3)):
            at_row = lo + m * ((k + later) % 2)
            dst = region(c, p, 0, at_row, m)
            src = kv.at[pl.ds(at_row, m), pl.ds(256 * c, 256)] if p == 0 else dst
            found.append(send(c, p, k + 2 * later, src, dst, by, chunk))
        return found

    def passed(c, p, lo, n, chunk):
        m = n // 2
        r1 = region(c, p, 3, lo, m)
        r2 = region(c, p, 1, lo + m, m)
        return send(c, p, 4, r1, r1, 1, chunk), send(c, p, 5, r2, r2, 3, chunk)

    def begin(p, lo=0, n=256, chunk=0):
        for later in range(2):
            for c in range(3):
                for x in direct(c, p, lo, n, chunk, later):
                    x.start()

    def middle(p, lo=0, n=256, chunk=0):
        for c in range(3):
            for x, y in zip(direct(c, p, lo, n, chunk, 0), passed(c, p, lo, n, chunk)):
                x.wait_recv()
                y.start()

    def end(p, lo=0, n=256, chunk=0):
        for c in range(3):
            for x in (*direct(c, p, lo, n, chunk, 1), *passed(c, p, lo, n, chunk)):
                x.wait_recv()

    def drain(p, lo=0, n=256, chunk=0):
        for c in range(3):
            for later in range(2):
                for x in direct(c, p, lo, n, chunk, later):
                    x.wait_send()
            for x in passed(c, p, lo, n, chunk):
                x.wait_send()

    def queries(k, src, dst):
        return pltpu.make_async_remote_copy(
            src_ref=src.at[pl.ds((1 - half) * TQ, TQ), :], dst_ref=dst, send_sem=qs.at[k],
            recv_sem=qr.at[k], device_id=(mirror, tp), device_id_type=MESH,
        )

    qcopies = (queries(0, qn_in, qgot_n), queries(1, qw_in, qgot_w))
    begin(0)
    middle(0)
    own.wait()
    end(0)
    begin(1)
    for x in qcopies:
        x.start()
    middle(1)
    end(1)
    begin(2, *CHUNKS[0], 0)

    for x in qcopies:
        x.wait_recv()
    lane = lax.broadcasted_iota(jnp.int32, (TQ, 128), 1)
    zero = jnp.zeros((TQ, 128), jnp.bfloat16)
    for mine in (1, 0):
        tile = 1 - half if mine else half
        for h in range(4):
            col = slice(h * 128, (h + 1) * 128)
            rows = qn_in[pl.ds(half * TQ, TQ), col] if mine else qgot_n[:, col]
            qn[tile, h * TQ : (h + 1) * TQ, :] = jnp.where(lane < 64, rows, zero)
            qn[tile, (4 + h) * TQ : (5 + h) * TQ, :] = jnp.where(lane < 64, zero, rows)
        for h in range(2):
            for m in range(2):
                col = slice(h * 256 + m * 128, h * 256 + (m + 1) * 128)
                rows = qw_in[pl.ds(half * TQ, TQ), col] if mine else qgot_w[:, col]
                put = slice((2 * m + h) * TQ, (2 * m + h + 1) * TQ)
                qw[tile, put, m * 128 : (m + 1) * 128] = rows
                qw[tile, put, (1 - m) * 128 : (2 - m) * 128] = zero
    mn[...] = jnp.full(mn.shape, -1e30, jnp.float32)
    mw[...] = jnp.full(mw.shape, -1e30, jnp.float32)
    accn[...] = jnp.zeros(accn.shape, jnp.float32)
    accw[...] = jnp.zeros(accw.shape, jnp.float32)
    lw[...] = jnp.zeros(lw.shape, jnp.float32)

    middle(2, *CHUNKS[0], 0)
    begin(2, *CHUNKS[1], 1)

    low = half * mirror + (1 - half) * sp
    high = 63 - low

    def place(s):
        after = [(s >= start).astype(jnp.int32) for start in STARTS]
        j = s - sum(SPANS[k - 1] * after[k] for k in range(1, len(CHUNKS)))
        width = 16 + 16 * after[3]
        n_hi = high // width + 1
        n_lo = low // width + 1
        turned = half * after[4]
        first = n_hi * (1 - turned) + n_lo * turned
        second = (j >= first).astype(jnp.int32)
        tile = turned + second - 2 * turned * second
        g = j - second * first
        last = n_hi * (1 - tile) + n_lo * tile - 1
        row = sum((CHUNKS[k][0] - CHUNKS[k - 1][0]) * after[k] for k in range(1, len(CHUNKS)))
        return after, row, tile, g, g == last, g * width * 256 + row

    def fetch(s, slot):
        after, row, _, g, _, _ = place(s)

        @pl.when(after[3] == 0)
        def _():
            for k in range(16):
                pltpu.make_async_copy(
                    kvall.at[g, k // 4, k % 4, pl.ds(pl.multiple_of(row, 32), 64), :],
                    buf.at[slot, k // 4, pl.ds((k % 4) * 64, 64), :], bsem.at[slot],
                ).start()

        @pl.when(after[3] == 1)
        def _():
            for k in range(32):
                pltpu.make_async_copy(
                    kvall.at[2 * g + k // 16, k // 4 % 4, k % 4, pl.ds(pl.multiple_of(row, 32), 32), :],
                    buf.at[slot, k // 8, pl.ds((k % 8) * 32, 32), :], bsem.at[slot],
                ).start()

    def finish(tile):
        for h in range(4):
            r0, r1 = h * TQ, (4 + h) * TQ
            d = accn[tile, r0 : r0 + TQ, 0:128] / accn[tile, r0 : r0 + TQ, 128:256] - lamn[h] * (
                accn[tile, r1 : r1 + TQ, 0:128] / accn[tile, r1 : r1 + TQ, 128:256]
            )
            d = d * lax.rsqrt(jnp.mean(d * d, axis=-1, keepdims=True) + EPS) * gn[...]
            att[tile, :, h * 128 : (h + 1) * 128] = d.astype(jnp.bfloat16)
        for h in range(2):
            r0, r1 = h * TQ, (2 + h) * TQ
            l0 = jnp.sum(lw[tile, r0 : r0 + TQ, :], axis=-1, keepdims=True)
            l1 = jnp.sum(lw[tile, r1 : r1 + TQ, :], axis=-1, keepdims=True)
            d = accw[tile, r0 : r0 + TQ, :] / l0 - lamw[h] * (accw[tile, r1 : r1 + TQ, :] / l1)
            d = d * lax.rsqrt(jnp.mean(d * d, axis=-1, keepdims=True) + EPS) * gw[...]
            att[tile, :, 512 + h * 256 : 512 + (h + 1) * 256] = d.astype(jnp.bfloat16)

    def deliver(k, tile, who):
        return pltpu.make_async_remote_copy(
            src_ref=att.at[tile], dst_ref=fin.at[tp], send_sem=ds.at[k], recv_sem=dr.at[tp],
            device_id=who, device_id_type=MESH,
        )

    def step(s, carry):
        slot = s % 2
        after, _, tile, g, masked, first_key = place(s)
        for chunk in range(len(CHUNKS)):
            @pl.when(s == STARTS[chunk])
            def _():
                end(2, *CHUNKS[chunk], chunk)
                fetch(s, slot)
        for chunk, turn in TURNS.items():
            @pl.when(s == turn)
            def _():
                middle(2, *CHUNKS[chunk], chunk)
                if chunk + 1 < len(CHUNKS):
                    begin(2, *CHUNKS[chunk + 1], chunk + 1)

        @pl.when(s == STEPS - 1 - half)
        def _():
            finish(half)
            deliver(0, half, (mirror, half)).start()

        pltpu.make_async_copy(kvall.at[0, 0], buf.at[slot], bsem.at[slot]).wait()

        more = s + 1 < STEPS
        for start in STARTS[1:]:
            more = more & (s + 1 != start)

        @pl.when(more)
        def _():
            fetch(s + 1, 1 - slot)

        base = half * TQ + (high * (1 - tile) + low * tile) * 256

        def attend(mask):
            def columns(lo, n):
                return buf[slot, :, :, lo : lo + n].reshape(KEYS, n)

            keys_n, keys_w, vals_w = columns(0, 128), columns(256, 256), columns(512, 256)
            vals_n = jnp.concatenate(
                [columns(128, 128), jnp.ones((KEYS, 128), jnp.bfloat16)], axis=1
            )
            dims = (((1,), (1,)), ((), ()))
            if mask:
                row = lax.broadcasted_iota(jnp.int32, (RC, KEYS), 0) % TQ
                keep = (relpos[after[3]] + first_key) <= (row + base)

            def scores(narrow, r):
                if narrow:
                    return lax.dot_general(
                        qn[tile, r : r + RC, :], keys_n, dims, preferred_element_type=jnp.float32
                    )
                return lax.dot_general(
                    qw[tile, r : r + RC, :], keys_w, dims, preferred_element_type=jnp.float32
                )

            parts = [(True, r) for r in range(0, 8 * TQ, RC)]
            parts += [(False, r) for r in range(0, 4 * TQ, RC)]
            following = scores(*parts[0])
            for i, (narrow, r) in enumerate(parts):
                sc = following
                if i + 1 < len(parts):
                    following = scores(*parts[i + 1])
                m_ref = mn if narrow else mw
                sc = sc * ((64 if narrow else 128) ** -0.5 * LOG2E)
                if mask:
                    sc = jnp.where(keep, sc, -1e30)
                m_old = m_ref[tile, r : r + RC, :]
                m_new = jnp.maximum(m_old, jnp.max(sc, axis=-1, keepdims=True))
                m_ref[tile, r : r + RC, :] = m_new
                alpha = jnp.exp2(m_old - m_new)
                p = jnp.exp2(sc - jnp.tile(m_new, (1, KEYS // 128)))
                pb = p.astype(jnp.bfloat16)
                twice = jnp.tile(alpha, (1, 2))
                if narrow:
                    accn[tile, r : r + RC, :] = accn[tile, r : r + RC, :] * twice + jnp.dot(
                        pb, vals_n, preferred_element_type=jnp.float32
                    )
                else:
                    ps = p[:, 0:128]
                    for j in range(1, KEYS // 128):
                        ps = ps + p[:, j * 128 : (j + 1) * 128]
                    lw[tile, r : r + RC, :] = lw[tile, r : r + RC, :] * alpha + ps
                    accw[tile, r : r + RC, :] = accw[tile, r : r + RC, :] * twice + jnp.dot(
                        pb, vals_w, preferred_element_type=jnp.float32
                    )

        @pl.when(jnp.logical_not(masked))
        def _():
            attend(False)

        @pl.when(masked)
        def _():
            attend(True)

        return carry

    lax.fori_loop(0, STEPS, step, 0)

    finish(1 - half)

    @pl.when(tp != half)
    def _():
        deliver(1, 1 - half, (sp, 1 - tp)).start()

    drain(0)
    drain(1)
    for chunk in range(len(CHUNKS)):
        drain(2, *CHUNKS[chunk], chunk)
    for x in qcopies:
        x.wait_send()

    def arrived(slot):
        pltpu.make_async_remote_copy(
            src_ref=att.at[0], dst_ref=fin.at[slot], send_sem=ds.at[0], recv_sem=dr.at[slot],
            device_id=(mirror, half), device_id_type=MESH,
        ).wait_recv()

    @pl.when(tp == half)
    def _():
        arrived(1 - tp)
        out[pl.ds(tp, 1)] = att[pl.ds(1 - half, 1)]
        out[pl.ds(1 - tp, 1)] = fin[pl.ds(1 - tp, 1)]

    @pl.when(tp != half)
    def _():
        arrived(0)
        arrived(1)
        out[...] = fin[...]
        deliver(1, 1 - half, (sp, 1 - tp)).wait_send()

    deliver(0, half, (mirror, half)).wait_send()


def attention(qn, qw, kn, vn, kw, vw, lamn, lamw, gn, gw):
    col = np.arange(KEYS)
    rel = np.stack([(col // n) * 256 + col % n for n in (64, 32)]).astype(np.int32)
    vmem = pl.BlockSpec(memory_space=pltpu.VMEM)
    smem = pl.BlockSpec(memory_space=pltpu.SMEM)
    hbm = pl.BlockSpec(memory_space=pltpu.HBM)
    f32, bf16 = jnp.float32, jnp.bfloat16
    dma = pltpu.SemaphoreType.DMA
    _, out = pl.pallas_call(
        attn_kernel,
        in_specs=[vmem, vmem, hbm, hbm, hbm, hbm, smem, smem, vmem, vmem, vmem],
        out_specs=(hbm, vmem),
        out_shape=(
            jax.ShapeDtypeStruct((4, 4, 4, 256, 768), bf16),
            jax.ShapeDtypeStruct((2, TQ, 1024), bf16),
        ),
        scratch_shapes=[
            pltpu.VMEM((256, 768), bf16),
            pltpu.VMEM((2, 4, 256, 768), bf16),
            pltpu.VMEM((TQ, 512), bf16),
            pltpu.VMEM((TQ, 512), bf16),
            pltpu.VMEM((2, 8 * TQ, 128), bf16),
            pltpu.VMEM((2, 4 * TQ, 256), bf16),
            pltpu.VMEM((2, 8 * TQ, 128), f32),
            pltpu.VMEM((2, 4 * TQ, 128), f32),
            pltpu.VMEM((2, 8 * TQ, 256), f32),
            pltpu.VMEM((2, 4 * TQ, 256), f32),
            pltpu.VMEM((2, 4 * TQ, 128), f32),
            pltpu.VMEM((2, TQ, 1024), bf16),
            pltpu.VMEM((2, TQ, 1024), bf16),
            dma((4,)),
            dma,
            dma((2,)),
            dma((2,)),
            dma((126,)),
            dma((126,)),
            dma((2,)),
            dma((2,)),
            dma((2,)),
        ],
        compiler_params=pltpu.CompilerParams(
            collective_id=3, has_side_effects=True, vmem_limit_bytes=ATTN_BYTES
        ),
        cost_estimate=pl.CostEstimate(
            flops=30 * 10**9, bytes_accessed=60 * 10**6, transcendentals=0
        ),
        name="attention",
    )(
        qn, qw, kn, vn, kw, vw, lamn, lamw, gn.reshape(1, 128), gw.reshape(1, 256),
        jnp.asarray(rel.reshape(2, 1, KEYS)),
    )
    return out


def rms(v, gain):
    return v * lax.rsqrt(jnp.mean(v * v, axis=-1, keepdims=True) + EPS) * gain


def dot(a, b):
    return jnp.dot(a, b, preferred_element_type=jnp.float32)


def ranks(ids):
    expert = lax.broadcasted_iota(jnp.int32, (EXPERTS, TQ), 0)
    named = jnp.zeros((EXPERTS, TQ), jnp.float32)
    for k in range(TOPK):
        named = named + (ids[k : k + 1, :] == expert).astype(jnp.float32)
    before = lax.broadcasted_iota(jnp.int32, (TQ, TQ), 0) < lax.broadcasted_iota(
        jnp.int32, (TQ, TQ), 1
    )
    count = dot(named.astype(jnp.bfloat16), before.astype(jnp.bfloat16))
    return (named * (count + 1.0)).astype(jnp.bfloat16)


def mid_kernel(
    f, on_in, ow_in, stream, gmix, gffn, ids, rank_of, piece_mask, mixed_out, normed_out, slab,
    on, ow, picks, sems,
):
    loads = []
    for i, (src, dst) in enumerate(((on_in, on), (ow_in, ow))):
        copy = pltpu.make_async_copy(src, dst, sems.at[i])
        copy.start()
        loads.append(copy)
    value = ranks(ids[...])
    row = lax.broadcasted_iota(jnp.int32, (GROUP_ROWS, EXPERTS), 0)
    lane = lax.broadcasted_iota(jnp.int32, (GROUP_ROWS, EXPERTS), 1)
    for g in range(EXPERTS // GROUP):
        low = (lane - g * GROUP) * SLAB
        spread = ((row >= low) & (row < low + SLAB)).astype(jnp.bfloat16)
        chosen = (dot(spread, value) == rank_of[...]).astype(jnp.float32).astype(jnp.bfloat16)
        chosen = jnp.concatenate([chosen] * PIECES, axis=1) * piece_mask[...]
        picks[g * GROUP_ROWS : (g + 1) * GROUP_ROWS, :] = chosen
    for copy in loads:
        copy.wait()
    projected = (
        dot(f[0, :, 0:512], on[0:512, :])
        + dot(f[1, :, 0:512], on[512:1024, :])
        + dot(f[0, :, 512:1024], ow[0:512, :])
        + dot(f[1, :, 512:1024], ow[512:1024, :])
    )
    mixed = (stream[...].astype(jnp.float32) + rms(projected, gmix[...])).astype(jnp.bfloat16)
    mixed_out[...] = mixed
    normed = rms(mixed.astype(jnp.float32), gffn[...]).astype(jnp.bfloat16)
    normed_out[...] = normed
    stacked = jnp.concatenate([normed[:, c * WIDTH : (c + 1) * WIDTH] for c in range(PIECES)], 0)

    def place_rows(g, carry):
        part = pl.ds(pl.multiple_of(g * GROUP_ROWS, GROUP_ROWS), GROUP_ROWS)
        slab[part, :] = dot(picks[part, :], stacked).astype(jnp.bfloat16)
        return carry

    lax.fori_loop(0, EXPERTS // GROUP, place_rows, 0, unroll=4)


def slab_tables():
    i = np.arange(GROUP_ROWS) % SLAB
    rank = np.broadcast_to((i % CAP + 1)[:, None], (GROUP_ROWS, EXPERTS)).astype(np.float32)
    piece = (i // CAP)[:, None] == (np.arange(PIECES * TQ) // TQ)[None, :]
    return rank, piece.astype(np.float32)


def order_table():
    i = np.arange(GROUP_ROWS)
    to = (i % SLAB // CAP) * (GROUP * CAP) + (i // SLAB) * CAP + i % CAP
    table = np.zeros((GROUP_ROWS, GROUP_ROWS), np.float32)
    table[to, i] = 1.0
    return table


def mid(f, on, ow, stream, gmix, gffn, ids):
    rank, piece = slab_tables()
    return pl.pallas_call(
        mid_kernel,
        in_specs=[VMEM, HBM, HBM, *[VMEM] * 6],
        scratch_shapes=[
            pltpu.VMEM((D // 2, D), jnp.bfloat16),
            pltpu.VMEM((D // 2, D), jnp.bfloat16),
            pltpu.VMEM((EXPERTS * SLAB, PIECES * TQ), jnp.bfloat16),
            pltpu.SemaphoreType.DMA((2,)),
        ],
        out_shape=(
            jax.ShapeDtypeStruct((TQ, D), jnp.bfloat16),
            jax.ShapeDtypeStruct((TQ, D), jnp.bfloat16),
            jax.ShapeDtypeStruct((EXPERTS * SLAB, WIDTH), jnp.bfloat16),
        ),
        compiler_params=pltpu.CompilerParams(vmem_limit_bytes=VMEM_BYTES),
        cost_estimate=pl.CostEstimate(flops=4 * 10**9, bytes_accessed=14 * 10**6, transcendentals=0),
        name="mid",
    )(
        f,
        on,
        ow,
        stream,
        gmix.reshape(1, D),
        gffn.reshape(1, D),
        ids,
        jnp.asarray(rank),
        jnp.asarray(piece, jnp.bfloat16),
    )


def expert_kernel(
    which, x, g1_in, u1_in, d1_in, g2_in, u2_in, d2_in, order, order_t, out,
    rows, results, g1, u1, d1, g2, u2, d2, sems,
):
    loads = []
    for i, (src, dst) in enumerate(
        (
            (g1_in.at[which[0]], g1),
            (u1_in.at[which[0]], u1),
            (d1_in.at[which[0]], d1),
            (g2_in.at[0], g2),
            (u2_in.at[0], u2),
            (d2_in.at[0], d2),
        )
    ):
        copy = pltpu.make_async_copy(src, dst, sems.at[i])
        copy.start()
        loads.append(copy)
    span = GROUP * CAP
    for g in range(EXPERTS // GROUP):
        got = dot(order[...], x[g * GROUP_ROWS : (g + 1) * GROUP_ROWS, :]).astype(jnp.bfloat16)
        for c in range(PIECES):
            rows[g * span : (g + 1) * span, c * WIDTH : (c + 1) * WIDTH] = got[
                c * span : (c + 1) * span, :
            ]
    for copy in loads:
        copy.wait()
    for m in range(0, EXPERTS * CAP, 256):
        part = rows[m : m + 256, :]
        total = None
        for gate, up, down in ((g1, u1, d1), (g2, u2, d2)):
            gated = dot(part, gate[...])
            hidden = (gated / (1.0 + jnp.exp(-gated)) * dot(part, up[...])).astype(jnp.bfloat16)
            term = dot(hidden, down[...])
            total = term if total is None else total + term
        results[m : m + 256, :] = total.astype(jnp.bfloat16)

    def give_back(g, carry):
        base = pl.multiple_of(g * span, span)
        stacked = jnp.concatenate(
            [results[pl.ds(base, span), c * WIDTH : (c + 1) * WIDTH] for c in range(PIECES)], 0
        )
        part = pl.ds(pl.multiple_of(g * GROUP_ROWS, GROUP_ROWS), GROUP_ROWS)
        out[part, :] = dot(order_t[...], stacked).astype(jnp.bfloat16)
        return carry

    lax.fori_loop(0, EXPERTS // GROUP, give_back, 0, unroll=4)


def run_expert(which, x, gate, up, down, gate2, up2, down2):
    table = order_table()
    full = lambda *shape: pl.BlockSpec(shape, lambda i, w: (0,) * len(shape))
    half = gate.shape[2]
    return pl.pallas_call(
        expert_kernel,
        grid_spec=pltpu.PrefetchScalarGridSpec(
            num_scalar_prefetch=1,
            grid=(1,),
            in_specs=[
                full(EXPERTS * SLAB, WIDTH),
                *[HBM] * 6,
                full(GROUP_ROWS, GROUP_ROWS),
                full(GROUP_ROWS, GROUP_ROWS),
            ],
            out_specs=full(EXPERTS * SLAB, WIDTH),
            scratch_shapes=[
                pltpu.VMEM((EXPERTS * CAP, D), jnp.bfloat16),
                pltpu.VMEM((EXPERTS * CAP, D), jnp.bfloat16),
                *[
                    pltpu.VMEM(shape, jnp.bfloat16)
                    for shape in ((D, half), (D, half), (half, D)) * 2
                ],
                pltpu.SemaphoreType.DMA((6,)),
            ],
        ),
        out_shape=jax.ShapeDtypeStruct((EXPERTS * SLAB, WIDTH), jnp.bfloat16),
        compiler_params=pltpu.CompilerParams(vmem_limit_bytes=VMEM_BYTES),
        cost_estimate=pl.CostEstimate(flops=6 * 10**9, bytes_accessed=14 * 10**6, transcendentals=0),
        name="expert",
    )(
        which,
        x,
        gate,
        up,
        down,
        gate2,
        up2,
        down2,
        jnp.asarray(table, jnp.bfloat16),
        jnp.asarray(table.T, jnp.bfloat16),
    )


def combine_kernel(
    back_in, ids, weights, shared, mixed, gpost, rank_row, piece_row, out, back, sems
):
    loads = []
    for g in range(EXPERTS // GROUP):
        part = pl.ds(g * GROUP_ROWS, GROUP_ROWS)
        copy = pltpu.make_async_copy(back_in.at[part, :], back.at[part, :], sems.at[g])
        copy.start()
        loads.append(copy)
    value = ranks(ids[...])
    expert = lax.broadcasted_iota(jnp.int32, (EXPERTS, TQ), 0)
    share = jnp.zeros((EXPERTS, TQ), jnp.float32)
    for k in range(TOPK):
        share = share + jnp.where(ids[k : k + 1, :] == expert, weights[k : k + 1, :], 0.0)
    value = value.astype(jnp.float32).T.astype(jnp.bfloat16)
    share = share.T.astype(jnp.bfloat16)
    row = lax.broadcasted_iota(jnp.int32, (EXPERTS, GROUP_ROWS), 0)
    col = lax.broadcasted_iota(jnp.int32, (EXPERTS, GROUP_ROWS), 1)
    total = jnp.zeros((PIECES * TQ, WIDTH), jnp.float32)
    for g in range(EXPERTS // GROUP):
        low = (row - g * GROUP) * SLAB
        spread = ((col >= low) & (col < low + SLAB)).astype(jnp.bfloat16)
        held = jnp.where(dot(value, spread) == rank_row[...], dot(share, spread), 0.0)
        picks = jnp.concatenate(
            [jnp.where(piece_row[...] == float(c), held, 0.0) for c in range(PIECES)], 0
        ).astype(jnp.bfloat16)
        loads[g].wait()
        total = total + dot(picks, back[g * GROUP_ROWS : (g + 1) * GROUP_ROWS, :])
    routed = jnp.concatenate([total[c * TQ : (c + 1) * TQ, :] for c in range(PIECES)], axis=1)
    combined = shared[...] + routed
    out[...] = (mixed[...].astype(jnp.float32) + rms(combined, gpost[...])).astype(jnp.bfloat16)


def combine(back, ids, weights, shared, mixed, gpost):
    i = np.arange(GROUP_ROWS) % SLAB
    return pl.pallas_call(
        combine_kernel,
        in_specs=[HBM, *[VMEM] * 7],
        scratch_shapes=[
            pltpu.VMEM((EXPERTS * SLAB, WIDTH), jnp.bfloat16),
            pltpu.SemaphoreType.DMA((EXPERTS // GROUP,)),
        ],
        out_shape=jax.ShapeDtypeStruct((TQ, D), jnp.bfloat16),
        compiler_params=pltpu.CompilerParams(vmem_limit_bytes=VMEM_BYTES),
        cost_estimate=pl.CostEstimate(flops=3 * 10**9, bytes_accessed=6 * 10**6, transcendentals=0),
        name="combine",
    )(
        back,
        ids,
        weights,
        shared,
        mixed,
        gpost.reshape(1, D),
        jnp.asarray((i % CAP + 1)[None, :], jnp.float32),
        jnp.asarray((i // CAP)[None, :], jnp.float32),
    )


BOTH = ("sp", "tp")


def exchanged(slab):
    pieces = slab.reshape(EXPERTS, SLAB, WIDTH)
    return lax.all_to_all(pieces, BOTH, 0, 0, tiled=True).reshape(EXPERTS * SLAB, WIDTH)


def shards(
    queries_narrow,
    keys_narrow,
    values_narrow,
    queries_wide,
    keys_wide,
    values_wide,
    lambda_narrow,
    lambda_wide,
    gain_narrow,
    gain_wide,
    out_narrow,
    out_wide,
    stream,
    gain_mix,
    gain_ffn,
    gain_post,
    shared_gate,
    shared_up,
    shared_down,
    expert_gate,
    expert_up,
    expert_down,
    expert_ids,
    route_weights,
):
    tp = lax.axis_index("tp")
    across = [(0, 1), (1, 0)]
    other = [
        lax.ppermute(lax.dynamic_slice_in_dim(w, 1 - tp, 1, 0), "tp", across)
        for w in (expert_gate, expert_up, expert_down)
    ]
    attended = attention(
        queries_narrow,
        queries_wide,
        keys_narrow,
        values_narrow,
        keys_wide,
        values_wide,
        lambda_narrow,
        lambda_wide,
        gain_narrow,
        gain_wide,
    )
    mixed, normed, slab = mid(
        attended, out_narrow, out_wide, stream, gain_mix, gain_ffn, expert_ids.T
    )
    incoming = exchanged(slab)
    results = run_expert(
        jnp.reshape(tp, (1,)).astype(jnp.int32),
        incoming,
        expert_gate,
        expert_up,
        expert_down,
        *other,
    )
    back = exchanged(results)
    shared_hidden = (
        jax.nn.silu(dot(normed, shared_gate)) * dot(normed, shared_up)
    ).astype(jnp.bfloat16)
    shared_out = dot(shared_hidden, shared_down)
    return combine(back, expert_ids.T, route_weights.T, shared_out, mixed, gain_post)


def solution(mesh):
    return jax.shard_map(
        shards,
        mesh=mesh,
        in_specs=(
            P("sp", "tp"),
            P("sp", "tp"),
            P("sp", "tp"),
            P("sp", "tp"),
            P("sp", "tp"),
            P("sp", "tp"),
            P("tp"),
            P("tp"),
            P(),
            P(),
            P(),
            P(),
            P(("sp", "tp"), None),
            P(),
            P(),
            P(),
            P(),
            P(),
            P(),
            P("sp", None, "tp"),
            P("sp", None, "tp"),
            P("sp", "tp", None),
            P(("sp", "tp"), None),
            P(("sp", "tp"), None),
        ),
        out_specs=P(("sp", "tp"), None),
        check_vma=False,
    )
```

```python
import functools

import jax
import jax.numpy as jnp
import numpy as np
from jax import lax
from jax.experimental import pallas as pl
from jax.experimental.pallas import tpu as pltpu
from jax.sharding import PartitionSpec as P

D = 2048
TOPK = 4
EPS = 1e-06
TQ = 128
LOG2E = 1.4426950408889634
RC = 256
CAP = 6
PIECES = 4
WIDTH = D // PIECES
SLAB = PIECES * CAP
EXPERTS = 128
GROUP = 16
GROUP_ROWS = GROUP * SLAB
ATTN_BYTES = 60 * 2**20
VMEM_BYTES = 60 * 2**20
MESH = pl.DeviceIdType.MESH
VMEM = pl.BlockSpec(memory_space=pltpu.VMEM)
HBM = pl.BlockSpec(memory_space=pltpu.HBM)
ORDERS = ((0, 1, 2), (1, 2, 0), (2, 0, 1))
STRIDE = (1, 4, 16)

CHUNKS = ((0, 64), (64, 64), (128, 64), (192, 32), (224, 32))
SPANS = (5, 5, 5, 3, 3)
STARTS = (0, 5, 10, 15, 18)
STEPS = 21
TURNS = {1: 2, 2: 7, 3: 11, 4: 14}
KEYS = 1024


def attn_kernel(
    qn_in, qw_in, kn_in, vn_in, kw_in, vw_in, lamn, lamw, gn, gw, relpos,
    kvall, out,
    kv, buf, qgot_n, qgot_w, qn, qw, mn, mw, accn, accw, lw, att, fin,
    isem, osem, qs, qr, ssem, rsem, bsem, ds, dr,
):
    sp = lax.axis_index("sp")
    tp = lax.axis_index("tp")
    half = sp // 32
    at = (sp % 4, (sp // 4) % 4, sp // 16)
    mirror = 63 - sp

    def dev(d, by):
        return (sp + ((at[d] + by) % 4 - at[d]) * STRIDE[d], tp)

    loads = []
    for i, (src, lo, n) in enumerate(
        ((kn_in, 0, 128), (vn_in, 128, 128), (kw_in, 256, 256), (vw_in, 512, 256))
    ):
        copy = pltpu.make_async_copy(src, kv.at[:, pl.ds(lo, n)], isem.at[i])
        copy.start()
        loads.append(copy)

    barrier = pltpu.get_barrier_semaphore()
    for d in range(3):
        for by in (1, 3):
            pl.semaphore_signal(barrier, inc=1, device_id=dev(d, by), device_id_type=MESH)
    for who in ((sp, 1 - tp), (mirror, tp), (mirror, 1 - tp)):
        pl.semaphore_signal(barrier, inc=1, device_id=who, device_id_type=MESH)
    pl.semaphore_wait(barrier, 9)
    for copy in loads:
        copy.wait()
    own = pltpu.make_async_copy(kv, kvall.at[at[2], at[1], at[0]], osem)
    own.start()

    def region(c, p, shift, lo, n):
        order = ORDERS[c]
        idx = [at[0], at[1], at[2]]
        for d in order[:p]:
            idx[d] = slice(None)
        idx[order[p]] = (at[order[p]] + shift) % 4
        return kvall.at[idx[2], idx[1], idx[0], pl.ds(lo, n), pl.ds(256 * c, 256)]

    def send(c, p, k, src, dst, by, chunk=0):
        s = (c * 7 + p + chunk) * 6 + k
        return pltpu.make_async_remote_copy(
            src_ref=src, dst_ref=dst, send_sem=ssem.at[s], recv_sem=rsem.at[s],
            device_id=dev(ORDERS[c][p], by), device_id_type=MESH,
        )

    def direct(c, p, lo, n, chunk, later):
        m = n // 2
        found = []
        for k, by in ((0, 1), (1, 3)):
            at_row = lo + m * ((k + later) % 2)
            dst = region(c, p, 0, at_row, m)
            src = kv.at[pl.ds(at_row, m), pl.ds(256 * c, 256)] if p == 0 else dst
            found.append(send(c, p, k + 2 * later, src, dst, by, chunk))
        return found

    def passed(c, p, lo, n, chunk):
        m = n // 2
        r1 = region(c, p, 3, lo, m)
        r2 = region(c, p, 1, lo + m, m)
        return send(c, p, 4, r1, r1, 1, chunk), send(c, p, 5, r2, r2, 3, chunk)

    def begin(p, lo=0, n=256, chunk=0):
        for later in range(2):
            for c in range(3):
                for x in direct(c, p, lo, n, chunk, later):
                    x.start()

    def middle(p, lo=0, n=256, chunk=0):
        for c in range(3):
            for x, y in zip(direct(c, p, lo, n, chunk, 0), passed(c, p, lo, n, chunk)):
                x.wait_recv()
                y.start()

    def end(p, lo=0, n=256, chunk=0):
        for c in range(3):
            for x in (*direct(c, p, lo, n, chunk, 1), *passed(c, p, lo, n, chunk)):
                x.wait_recv()

    def drain(p, lo=0, n=256, chunk=0):
        for c in range(3):
            for later in range(2):
                for x in direct(c, p, lo, n, chunk, later):
                    x.wait_send()
            for x in passed(c, p, lo, n, chunk):
                x.wait_send()

    def queries(k, src, dst):
        return pltpu.make_async_remote_copy(
            src_ref=src.at[pl.ds((1 - half) * TQ, TQ), :], dst_ref=dst, send_sem=qs.at[k],
            recv_sem=qr.at[k], device_id=(mirror, tp), device_id_type=MESH,
        )

    qcopies = (queries(0, qn_in, qgot_n), queries(1, qw_in, qgot_w))
    begin(0)
    middle(0)
    own.wait()
    end(0)
    begin(1)
    for x in qcopies:
        x.start()
    middle(1)
    end(1)
    begin(2, *CHUNKS[0], 0)

    for x in qcopies:
        x.wait_recv()
    lane = lax.broadcasted_iota(jnp.int32, (TQ, 128), 1)
    zero = jnp.zeros((TQ, 128), jnp.bfloat16)
    for mine in (1, 0):
        tile = 1 - half if mine else half
        for h in range(4):
            col = slice(h * 128, (h + 1) * 128)
            rows = qn_in[pl.ds(half * TQ, TQ), col] if mine else qgot_n[:, col]
            qn[tile, h * TQ : (h + 1) * TQ, :] = jnp.where(lane < 64, rows, zero)
            qn[tile, (4 + h) * TQ : (5 + h) * TQ, :] = jnp.where(lane < 64, zero, rows)
        for h in range(2):
            for m in range(2):
                col = slice(h * 256 + m * 128, h * 256 + (m + 1) * 128)
                rows = qw_in[pl.ds(half * TQ, TQ), col] if mine else qgot_w[:, col]
                put = slice((2 * m + h) * TQ, (2 * m + h + 1) * TQ)
                qw[tile, put, m * 128 : (m + 1) * 128] = rows
                qw[tile, put, (1 - m) * 128 : (2 - m) * 128] = zero
    mn[...] = jnp.full(mn.shape, -1e30, jnp.float32)
    mw[...] = jnp.full(mw.shape, -1e30, jnp.float32)
    accn[...] = jnp.zeros(accn.shape, jnp.float32)
    accw[...] = jnp.zeros(accw.shape, jnp.float32)
    lw[...] = jnp.zeros(lw.shape, jnp.float32)

    middle(2, *CHUNKS[0], 0)
    begin(2, *CHUNKS[1], 1)

    low = half * mirror + (1 - half) * sp
    high = 63 - low

    def place(s):
        after = [(s >= start).astype(jnp.int32) for start in STARTS]
        j = s - sum(SPANS[k - 1] * after[k] for k in range(1, len(CHUNKS)))
        width = 16 + 16 * after[3]
        n_hi = high // width + 1
        n_lo = low // width + 1
        turned = half * after[4]
        first = n_hi * (1 - turned) + n_lo * turned
        second = (j >= first).astype(jnp.int32)
        tile = turned + second - 2 * turned * second
        g = j - second * first
        last = n_hi * (1 - tile) + n_lo * tile - 1
        row = sum((CHUNKS[k][0] - CHUNKS[k - 1][0]) * after[k] for k in range(1, len(CHUNKS)))
        return after, row, tile, g, g == last, g * width * 256 + row

    def fetch(s, slot):
        after, row, _, g, _, _ = place(s)

        @pl.when(after[3] == 0)
        def _():
            for k in range(16):
                pltpu.make_async_copy(
                    kvall.at[g, k // 4, k % 4, pl.ds(pl.multiple_of(row, 32), 64), :],
                    buf.at[slot, k // 4, pl.ds((k % 4) * 64, 64), :], bsem.at[slot],
                ).start()

        @pl.when(after[3] == 1)
        def _():
            for k in range(32):
                pltpu.make_async_copy(
                    kvall.at[2 * g + k // 16, k // 4 % 4, k % 4, pl.ds(pl.multiple_of(row, 32), 32), :],
                    buf.at[slot, k // 8, pl.ds((k % 8) * 32, 32), :], bsem.at[slot],
                ).start()

    def finish(tile):
        for h in range(4):
            r0, r1 = h * TQ, (4 + h) * TQ
            d = accn[tile, r0 : r0 + TQ, 0:128] / accn[tile, r0 : r0 + TQ, 128:256] - lamn[h] * (
                accn[tile, r1 : r1 + TQ, 0:128] / accn[tile, r1 : r1 + TQ, 128:256]
            )
            d = d * lax.rsqrt(jnp.mean(d * d, axis=-1, keepdims=True) + EPS) * gn[...]
            att[tile, :, h * 128 : (h + 1) * 128] = d.astype(jnp.bfloat16)
        for h in range(2):
            r0, r1 = h * TQ, (2 + h) * TQ
            l0 = jnp.sum(lw[tile, r0 : r0 + TQ, :], axis=-1, keepdims=True)
            l1 = jnp.sum(lw[tile, r1 : r1 + TQ, :], axis=-1, keepdims=True)
            d = accw[tile, r0 : r0 + TQ, :] / l0 - lamw[h] * (accw[tile, r1 : r1 + TQ, :] / l1)
            d = d * lax.rsqrt(jnp.mean(d * d, axis=-1, keepdims=True) + EPS) * gw[...]
            att[tile, :, 512 + h * 256 : 512 + (h + 1) * 256] = d.astype(jnp.bfloat16)

    def deliver(k, tile, who):
        return pltpu.make_async_remote_copy(
            src_ref=att.at[tile], dst_ref=fin.at[tp], send_sem=ds.at[k], recv_sem=dr.at[tp],
            device_id=who, device_id_type=MESH,
        )

    def step(s, carry):
        slot = s % 2
        after, _, tile, g, masked, first_key = place(s)
        for chunk in range(len(CHUNKS)):
            @pl.when(s == STARTS[chunk])
            def _():
                end(2, *CHUNKS[chunk], chunk)
        opening = s == STARTS[0]
        for start in STARTS[1:]:
            opening = opening | (s == start)

        @pl.when(opening)
        def _():
            fetch(s, slot)

        for chunk, turn in TURNS.items():
            @pl.when(s == turn)
            def _():
                middle(2, *CHUNKS[chunk], chunk)
                if chunk + 1 < len(CHUNKS):
                    begin(2, *CHUNKS[chunk + 1], chunk + 1)

        @pl.when(s == STEPS - 1 - half)
        def _():
            finish(half)
            deliver(0, half, (mirror, half)).start()

        pltpu.make_async_copy(kvall.at[0, 0], buf.at[slot], bsem.at[slot]).wait()

        more = s + 1 < STEPS
        for start in STARTS[1:]:
            more = more & (s + 1 != start)

        @pl.when(more)
        def _():
            fetch(s + 1, 1 - slot)

        base = half * TQ + (high * (1 - tile) + low * tile) * 256

        def attend(mask):
            def columns(lo, n):
                return buf[slot, :, :, lo : lo + n].reshape(KEYS, n)

            keys_n, keys_w, vals_w = columns(0, 128), columns(256, 256), columns(512, 256)
            vals_n = jnp.concatenate(
                [columns(128, 128), jnp.ones((KEYS, 128), jnp.bfloat16)], axis=1
            )
            dims = (((1,), (1,)), ((), ()))
            if mask:
                row = lax.broadcasted_iota(jnp.int32, (RC, KEYS), 0) % TQ
                keep = (relpos[after[3]] + first_key) <= (row + base)

            def scores(narrow, r):
                if narrow:
                    return lax.dot_general(
                        qn[tile, r : r + RC, :], keys_n, dims, preferred_element_type=jnp.float32
                    )
                return lax.dot_general(
                    qw[tile, r : r + RC, :], keys_w, dims, preferred_element_type=jnp.float32
                )

            parts = [(True, r) for r in range(0, 8 * TQ, RC)]
            parts += [(False, r) for r in range(0, 4 * TQ, RC)]
            following = scores(*parts[0])
            for i, (narrow, r) in enumerate(parts):
                sc = following
                if i + 1 < len(parts):
                    following = scores(*parts[i + 1])
                m_ref = mn if narrow else mw
                sc = sc * ((64 if narrow else 128) ** -0.5 * LOG2E)
                if mask:
                    sc = jnp.where(keep, sc, -1e30)
                m_old = m_ref[tile, r : r + RC, :]
                m_new = jnp.maximum(m_old, jnp.max(sc, axis=-1, keepdims=True))
                m_ref[tile, r : r + RC, :] = m_new
                alpha = jnp.exp2(m_old - m_new)
                p = jnp.exp2(sc - jnp.tile(m_new, (1, KEYS // 128)))
                pb = p.astype(jnp.bfloat16)
                twice = jnp.tile(alpha, (1, 2))
                if narrow:
                    accn[tile, r : r + RC, :] = accn[tile, r : r + RC, :] * twice + jnp.dot(
                        pb, vals_n, preferred_element_type=jnp.float32
                    )
                else:
                    ps = p[:, 0:128]
                    for j in range(1, KEYS // 128):
                        ps = ps + p[:, j * 128 : (j + 1) * 128]
                    lw[tile, r : r + RC, :] = lw[tile, r : r + RC, :] * alpha + ps
                    accw[tile, r : r + RC, :] = accw[tile, r : r + RC, :] * twice + jnp.dot(
                        pb, vals_w, preferred_element_type=jnp.float32
                    )

        @pl.when(jnp.logical_not(masked))
        def _():
            attend(False)

        @pl.when(masked)
        def _():
            attend(True)

        return carry

    lax.fori_loop(0, STEPS, step, 0)

    finish(1 - half)

    @pl.when(tp != half)
    def _():
        deliver(1, 1 - half, (sp, 1 - tp)).start()

    drain(0)
    drain(1)
    for chunk in range(len(CHUNKS)):
        drain(2, *CHUNKS[chunk], chunk)
    for x in qcopies:
        x.wait_send()

    def arrived(slot):
        pltpu.make_async_remote_copy(
            src_ref=att.at[0], dst_ref=fin.at[slot], send_sem=ds.at[0], recv_sem=dr.at[slot],
            device_id=(mirror, half), device_id_type=MESH,
        ).wait_recv()

    @pl.when(tp == half)
    def _():
        arrived(1 - tp)
        out[pl.ds(tp, 1)] = att[pl.ds(1 - half, 1)]
        out[pl.ds(1 - tp, 1)] = fin[pl.ds(1 - tp, 1)]

    @pl.when(tp != half)
    def _():
        arrived(0)
        arrived(1)
        out[...] = fin[...]
        deliver(1, 1 - half, (sp, 1 - tp)).wait_send()

    deliver(0, half, (mirror, half)).wait_send()


def attention(qn, qw, kn, vn, kw, vw, lamn, lamw, gn, gw):
    col = np.arange(KEYS)
    rel = np.stack([(col // n) * 256 + col % n for n in (64, 32)]).astype(np.int32)
    vmem = pl.BlockSpec(memory_space=pltpu.VMEM)
    smem = pl.BlockSpec(memory_space=pltpu.SMEM)
    hbm = pl.BlockSpec(memory_space=pltpu.HBM)
    f32, bf16 = jnp.float32, jnp.bfloat16
    dma = pltpu.SemaphoreType.DMA
    _, out = pl.pallas_call(
        attn_kernel,
        in_specs=[vmem, vmem, hbm, hbm, hbm, hbm, smem, smem, vmem, vmem, vmem],
        out_specs=(hbm, vmem),
        out_shape=(
            jax.ShapeDtypeStruct((4, 4, 4, 256, 768), bf16),
            jax.ShapeDtypeStruct((2, TQ, 1024), bf16),
        ),
        scratch_shapes=[
            pltpu.VMEM((256, 768), bf16),
            pltpu.VMEM((2, 4, 256, 768), bf16),
            pltpu.VMEM((TQ, 512), bf16),
            pltpu.VMEM((TQ, 512), bf16),
            pltpu.VMEM((2, 8 * TQ, 128), bf16),
            pltpu.VMEM((2, 4 * TQ, 256), bf16),
            pltpu.VMEM((2, 8 * TQ, 128), f32),
            pltpu.VMEM((2, 4 * TQ, 128), f32),
            pltpu.VMEM((2, 8 * TQ, 256), f32),
            pltpu.VMEM((2, 4 * TQ, 256), f32),
            pltpu.VMEM((2, 4 * TQ, 128), f32),
            pltpu.VMEM((2, TQ, 1024), bf16),
            pltpu.VMEM((2, TQ, 1024), bf16),
            dma((4,)),
            dma,
            dma((2,)),
            dma((2,)),
            dma((126,)),
            dma((126,)),
            dma((2,)),
            dma((2,)),
            dma((2,)),
        ],
        compiler_params=pltpu.CompilerParams(
            collective_id=3, has_side_effects=True, vmem_limit_bytes=ATTN_BYTES
        ),
        cost_estimate=pl.CostEstimate(
            flops=30 * 10**9, bytes_accessed=60 * 10**6, transcendentals=0
        ),
        name="attention",
    )(
        qn, qw, kn, vn, kw, vw, lamn, lamw, gn.reshape(1, 128), gw.reshape(1, 256),
        jnp.asarray(rel.reshape(2, 1, KEYS)),
    )
    return out


def rms(v, gain):
    return v * lax.rsqrt(jnp.mean(v * v, axis=-1, keepdims=True) + EPS) * gain


def dot(a, b):
    return jnp.dot(a, b, preferred_element_type=jnp.float32)


def ranks(ids):
    expert = lax.broadcasted_iota(jnp.int32, (EXPERTS, TQ), 0)
    named = jnp.zeros((EXPERTS, TQ), jnp.float32)
    for k in range(TOPK):
        named = named + (ids[k : k + 1, :] == expert).astype(jnp.float32)
    before = lax.broadcasted_iota(jnp.int32, (TQ, TQ), 0) < lax.broadcasted_iota(
        jnp.int32, (TQ, TQ), 1
    )
    count = dot(named.astype(jnp.bfloat16), before.astype(jnp.bfloat16))
    return (named * (count + 1.0)).astype(jnp.bfloat16)


def mid_kernel(
    f, on_in, ow_in, stream, gmix, gffn, ids, rank_of, piece_mask, mixed_out, normed_out, slab,
    on, ow, picks, sems,
):
    loads = []
    for i, (src, dst) in enumerate(((on_in, on), (ow_in, ow))):
        copy = pltpu.make_async_copy(src, dst, sems.at[i])
        copy.start()
        loads.append(copy)
    value = ranks(ids[...])
    row = lax.broadcasted_iota(jnp.int32, (GROUP_ROWS, EXPERTS), 0)
    lane = lax.broadcasted_iota(jnp.int32, (GROUP_ROWS, EXPERTS), 1)
    for g in range(EXPERTS // GROUP):
        low = (lane - g * GROUP) * SLAB
        spread = ((row >= low) & (row < low + SLAB)).astype(jnp.bfloat16)
        chosen = (dot(spread, value) == rank_of[...]).astype(jnp.float32).astype(jnp.bfloat16)
        chosen = jnp.concatenate([chosen] * PIECES, axis=1) * piece_mask[...]
        picks[g * GROUP_ROWS : (g + 1) * GROUP_ROWS, :] = chosen
    for copy in loads:
        copy.wait()
    projected = (
        dot(f[0, :, 0:512], on[0:512, :])
        + dot(f[1, :, 0:512], on[512:1024, :])
        + dot(f[0, :, 512:1024], ow[0:512, :])
        + dot(f[1, :, 512:1024], ow[512:1024, :])
    )
    mixed = (stream[...].astype(jnp.float32) + rms(projected, gmix[...])).astype(jnp.bfloat16)
    mixed_out[...] = mixed
    normed = rms(mixed.astype(jnp.float32), gffn[...]).astype(jnp.bfloat16)
    normed_out[...] = normed
    stacked = jnp.concatenate([normed[:, c * WIDTH : (c + 1) * WIDTH] for c in range(PIECES)], 0)

    def place_rows(g, carry):
        part = pl.ds(pl.multiple_of(g * GROUP_ROWS, GROUP_ROWS), GROUP_ROWS)
        slab[part, :] = dot(picks[part, :], stacked).astype(jnp.bfloat16)
        return carry

    lax.fori_loop(0, EXPERTS // GROUP, place_rows, 0, unroll=8)


def slab_tables():
    i = np.arange(GROUP_ROWS) % SLAB
    rank = np.broadcast_to((i % CAP + 1)[:, None], (GROUP_ROWS, EXPERTS)).astype(np.float32)
    piece = (i // CAP)[:, None] == (np.arange(PIECES * TQ) // TQ)[None, :]
    return rank, piece.astype(np.float32)


def order_table():
    i = np.arange(GROUP_ROWS)
    to = (i % SLAB // CAP) * (GROUP * CAP) + (i // SLAB) * CAP + i % CAP
    table = np.zeros((GROUP_ROWS, GROUP_ROWS), np.float32)
    table[to, i] = 1.0
    return table


def mid(f, on, ow, stream, gmix, gffn, ids):
    rank, piece = slab_tables()
    return pl.pallas_call(
        mid_kernel,
        in_specs=[VMEM, HBM, HBM, *[VMEM] * 6],
        scratch_shapes=[
            pltpu.VMEM((D // 2, D), jnp.bfloat16),
            pltpu.VMEM((D // 2, D), jnp.bfloat16),
            pltpu.VMEM((EXPERTS * SLAB, PIECES * TQ), jnp.bfloat16),
            pltpu.SemaphoreType.DMA((2,)),
        ],
        out_shape=(
            jax.ShapeDtypeStruct((TQ, D), jnp.bfloat16),
            jax.ShapeDtypeStruct((TQ, D), jnp.bfloat16),
            jax.ShapeDtypeStruct((EXPERTS * SLAB, WIDTH), jnp.bfloat16),
        ),
        compiler_params=pltpu.CompilerParams(vmem_limit_bytes=VMEM_BYTES),
        cost_estimate=pl.CostEstimate(flops=4 * 10**9, bytes_accessed=14 * 10**6, transcendentals=0),
        name="mid",
    )(
        f,
        on,
        ow,
        stream,
        gmix.reshape(1, D),
        gffn.reshape(1, D),
        ids,
        jnp.asarray(rank),
        jnp.asarray(piece, jnp.bfloat16),
    )


def expert_kernel(
    which, x, g1_in, u1_in, d1_in, g2_in, u2_in, d2_in, order, order_t, out,
    rows, results, g1, u1, d1, g2, u2, d2, sems,
):
    loads = []
    for i, (src, dst) in enumerate(
        (
            (g1_in.at[which[0]], g1),
            (u1_in.at[which[0]], u1),
            (d1_in.at[which[0]], d1),
            (g2_in.at[0], g2),
            (u2_in.at[0], u2),
            (d2_in.at[0], d2),
        )
    ):
        copy = pltpu.make_async_copy(src, dst, sems.at[i])
        copy.start()
        loads.append(copy)
    span = GROUP * CAP
    for g in range(EXPERTS // GROUP):
        got = dot(order[...], x[g * GROUP_ROWS : (g + 1) * GROUP_ROWS, :]).astype(jnp.bfloat16)
        for c in range(PIECES):
            rows[g * span : (g + 1) * span, c * WIDTH : (c + 1) * WIDTH] = got[
                c * span : (c + 1) * span, :
            ]
    for copy in loads:
        copy.wait()
    for m in range(0, EXPERTS * CAP, 256):
        part = rows[m : m + 256, :]
        total = None
        for gate, up, down in ((g1, u1, d1), (g2, u2, d2)):
            gated = dot(part, gate[...])
            hidden = (gated / (1.0 + jnp.exp(-gated)) * dot(part, up[...])).astype(jnp.bfloat16)
            term = dot(hidden, down[...])
            total = term if total is None else total + term
        results[m : m + 256, :] = total.astype(jnp.bfloat16)

    def give_back(g, carry):
        base = pl.multiple_of(g * span, span)
        stacked = jnp.concatenate(
            [results[pl.ds(base, span), c * WIDTH : (c + 1) * WIDTH] for c in range(PIECES)], 0
        )
        part = pl.ds(pl.multiple_of(g * GROUP_ROWS, GROUP_ROWS), GROUP_ROWS)
        out[part, :] = dot(order_t[...], stacked).astype(jnp.bfloat16)
        return carry

    lax.fori_loop(0, EXPERTS // GROUP, give_back, 0, unroll=8)


def run_expert(which, x, gate, up, down, gate2, up2, down2):
    table = order_table()
    full = lambda *shape: pl.BlockSpec(shape, lambda i, w: (0,) * len(shape))
    half = gate.shape[2]
    return pl.pallas_call(
        expert_kernel,
        grid_spec=pltpu.PrefetchScalarGridSpec(
            num_scalar_prefetch=1,
            grid=(1,),
            in_specs=[
                full(EXPERTS * SLAB, WIDTH),
                *[HBM] * 6,
                full(GROUP_ROWS, GROUP_ROWS),
                full(GROUP_ROWS, GROUP_ROWS),
            ],
            out_specs=full(EXPERTS * SLAB, WIDTH),
            scratch_shapes=[
                pltpu.VMEM((EXPERTS * CAP, D), jnp.bfloat16),
                pltpu.VMEM((EXPERTS * CAP, D), jnp.bfloat16),
                *[
                    pltpu.VMEM(shape, jnp.bfloat16)
                    for shape in ((D, half), (D, half), (half, D)) * 2
                ],
                pltpu.SemaphoreType.DMA((6,)),
            ],
        ),
        out_shape=jax.ShapeDtypeStruct((EXPERTS * SLAB, WIDTH), jnp.bfloat16),
        compiler_params=pltpu.CompilerParams(vmem_limit_bytes=VMEM_BYTES),
        cost_estimate=pl.CostEstimate(flops=6 * 10**9, bytes_accessed=14 * 10**6, transcendentals=0),
        name="expert",
    )(
        which,
        x,
        gate,
        up,
        down,
        gate2,
        up2,
        down2,
        jnp.asarray(table, jnp.bfloat16),
        jnp.asarray(table.T, jnp.bfloat16),
    )


def combine_kernel(
    back_in, ids, weights, shared, mixed, gpost, rank_row, piece_row, out, back, sems
):
    loads = []
    for g in range(EXPERTS // GROUP):
        part = pl.ds(g * GROUP_ROWS, GROUP_ROWS)
        copy = pltpu.make_async_copy(back_in.at[part, :], back.at[part, :], sems.at[g])
        copy.start()
        loads.append(copy)
    value = ranks(ids[...])
    expert = lax.broadcasted_iota(jnp.int32, (EXPERTS, TQ), 0)
    share = jnp.zeros((EXPERTS, TQ), jnp.float32)
    for k in range(TOPK):
        share = share + jnp.where(ids[k : k + 1, :] == expert, weights[k : k + 1, :], 0.0)
    value = value.astype(jnp.float32).T.astype(jnp.bfloat16)
    share = share.T.astype(jnp.bfloat16)
    row = lax.broadcasted_iota(jnp.int32, (EXPERTS, GROUP_ROWS), 0)
    col = lax.broadcasted_iota(jnp.int32, (EXPERTS, GROUP_ROWS), 1)
    total = jnp.zeros((PIECES * TQ, WIDTH), jnp.float32)
    for g in range(EXPERTS // GROUP):
        low = (row - g * GROUP) * SLAB
        spread = ((col >= low) & (col < low + SLAB)).astype(jnp.bfloat16)
        held = jnp.where(dot(value, spread) == rank_row[...], dot(share, spread), 0.0)
        picks = jnp.concatenate(
            [jnp.where(piece_row[...] == float(c), held, 0.0) for c in range(PIECES)], 0
        ).astype(jnp.bfloat16)
        loads[g].wait()
        total = total + dot(picks, back[g * GROUP_ROWS : (g + 1) * GROUP_ROWS, :])
    routed = jnp.concatenate([total[c * TQ : (c + 1) * TQ, :] for c in range(PIECES)], axis=1)
    combined = shared[...] + routed
    out[...] = (mixed[...].astype(jnp.float32) + rms(combined, gpost[...])).astype(jnp.bfloat16)


def combine(back, ids, weights, shared, mixed, gpost):
    i = np.arange(GROUP_ROWS) % SLAB
    return pl.pallas_call(
        combine_kernel,
        in_specs=[HBM, *[VMEM] * 7],
        scratch_shapes=[
            pltpu.VMEM((EXPERTS * SLAB, WIDTH), jnp.bfloat16),
            pltpu.SemaphoreType.DMA((EXPERTS // GROUP,)),
        ],
        out_shape=jax.ShapeDtypeStruct((TQ, D), jnp.bfloat16),
        compiler_params=pltpu.CompilerParams(vmem_limit_bytes=VMEM_BYTES),
        cost_estimate=pl.CostEstimate(flops=3 * 10**9, bytes_accessed=6 * 10**6, transcendentals=0),
        name="combine",
    )(
        back,
        ids,
        weights,
        shared,
        mixed,
        gpost.reshape(1, D),
        jnp.asarray((i % CAP + 1)[None, :], jnp.float32),
        jnp.asarray((i // CAP)[None, :], jnp.float32),
    )


BOTH = ("sp", "tp")


def exchanged(slab):
    pieces = slab.reshape(EXPERTS, SLAB, WIDTH)
    return lax.all_to_all(pieces, BOTH, 0, 0, tiled=True).reshape(EXPERTS * SLAB, WIDTH)


def shards(
    queries_narrow,
    keys_narrow,
    values_narrow,
    queries_wide,
    keys_wide,
    values_wide,
    lambda_narrow,
    lambda_wide,
    gain_narrow,
    gain_wide,
    out_narrow,
    out_wide,
    stream,
    gain_mix,
    gain_ffn,
    gain_post,
    shared_gate,
    shared_up,
    shared_down,
    expert_gate,
    expert_up,
    expert_down,
    expert_ids,
    route_weights,
):
    tp = lax.axis_index("tp")
    across = [(0, 1), (1, 0)]
    other = [
        lax.ppermute(lax.dynamic_slice_in_dim(w, 1 - tp, 1, 0), "tp", across)
        for w in (expert_gate, expert_up, expert_down)
    ]
    attended = attention(
        queries_narrow,
        queries_wide,
        keys_narrow,
        values_narrow,
        keys_wide,
        values_wide,
        lambda_narrow,
        lambda_wide,
        gain_narrow,
        gain_wide,
    )
    mixed, normed, slab = mid(
        attended, out_narrow, out_wide, stream, gain_mix, gain_ffn, expert_ids.T
    )
    incoming = exchanged(slab)
    results = run_expert(
        jnp.reshape(tp, (1,)).astype(jnp.int32),
        incoming,
        expert_gate,
        expert_up,
        expert_down,
        *other,
    )
    back = exchanged(results)
    shared_hidden = (
        jax.nn.silu(dot(normed, shared_gate)) * dot(normed, shared_up)
    ).astype(jnp.bfloat16)
    shared_out = dot(shared_hidden, shared_down)
    return combine(back, expert_ids.T, route_weights.T, shared_out, mixed, gain_post)


def solution(mesh):
    return jax.shard_map(
        shards,
        mesh=mesh,
        in_specs=(
            P("sp", "tp"),
            P("sp", "tp"),
            P("sp", "tp"),
            P("sp", "tp"),
            P("sp", "tp"),
            P("sp", "tp"),
            P("tp"),
            P("tp"),
            P(),
            P(),
            P(),
            P(),
            P(("sp", "tp"), None),
            P(),
            P(),
            P(),
            P(),
            P(),
            P(),
            P("sp", None, "tp"),
            P("sp", None, "tp"),
            P("sp", "tp", None),
            P(("sp", "tp"), None),
            P(("sp", "tp"), None),
        ),
        out_specs=P(("sp", "tp"), None),
        check_vma=False,
    )
```
